32 devices in a mesh: grp: 2 (over y), sp: 4 (over z), tp: 4 (over x, core).
Axes of the slice: x: 2, y: 2, z: 4, core: 2. Of those that a mesh axis runs over, the one named last changes fastest.
Arguments:
- tokens: bfloat16 [1024, 2048], P(('grp', 'sp'), 'tp'), parts along dimension 0, may hold values from -6 to 6
- norm_gain: float32 [2048], replicated, may hold values from 0.1 to 1.9
- att_q_weight: bfloat16 [1024, 2048], P('tp', 'sp'), may hold values from -0.625 to 0.625
- att_k_weight: bfloat16 [512, 2048], P('tp', 'sp'), may hold values from -0.125 to 0.125
- att_v_weight: bfloat16 [512, 2048], P('tp', 'sp'), may hold values from -0.125 to 0.125
- rec_q_weight: bfloat16 [1024, 2048], P('tp', 'sp'), may hold values from -0.125 to 0.125
- rec_f_weight: bfloat16 [1024, 2048], P('tp', 'sp'), may hold values from -0.125 to 0.125
- rec_i_weight: bfloat16 [1024, 2048], P('tp', 'sp'), may hold values from -0.125 to 0.125
- att_out_weight: bfloat16 [1024, 2048], P('tp', 'sp'), may hold values from -1.5 to 1.5
- rec_out_weight: bfloat16 [1024, 2048], P('tp', 'sp'), may hold values from -0.1875 to 0.1875
- score_offset: float32 [16], P('tp'), may hold values from -11.5 to -3
- lower_bound: float32 [1024], P('tp'), may hold values from 0.94 to 0.99999
- decay_shift: float32 [1024, 1024], P(('grp', 'sp'), 'tp'), parts along dimension 0, may hold values from -2.1 to 0
- rec_gain: float32 [1024], P('tp'), may hold values from 0.1 to 1.9
Outputs:
- mixed: bfloat16 [1024, 2048], P(('grp', 'sp', 'tp')), parts along dimension 0
The draws below stay inside these ranges and needn't reach their ends.
There are 2 independent parts, one for each index of `grp`. The reference program is written for one: setup_inputs(seed, part) draws one part's arguments, and reference() takes and returns one part's arrays. A program takes and returns all parts, laid end to end along the dimension named above; an argument that names none is the same for every part. Nothing has to cross between parts.
All inputs are finite; a program needn't handle non-finite values.
Results may differ from the reference program's by a relative error of at most 0.015.
Values may be sent and summed in bfloat16 or wider, within the bound.
A program may use at most 64 MiB of HBM per device.

```python
import math
import jax
import jax.numpy as jnp
from jax import lax

D = 2048
ATT_HEADS = 16
KV_HEADS = 8
HEAD = 64
RECURRENT_COUNT = 8
REC_KEY = 128
REC_VAL = 128
SPAN = 64
TOK_DEV = 128
SEQ = 512
ATT_WIDTH = 1024
KV_WIDTH = 512
KEY_WIDTH = 1024
VAL_WIDTH = 1024
N_TP = 4


def draw_score_offset(key, part):
    order = jax.random.permutation(jax.random.fold_in(key, 11), ATT_HEADS)
    level = jax.random.uniform(jax.random.fold_in(key, 12), (ATT_HEADS,), jnp.float32)
    slow = order >= ATT_HEADS // 2
    far = -11.5 + 1.5 * level
    near = -6.0 + 3.0 * level
    return jnp.where(slow, far, near).astype(jnp.float32)


def draw_lower_bound(key, part):
    order = jax.random.permutation(jax.random.fold_in(key, 21), RECURRENT_COUNT)
    slow = order >= RECURRENT_COUNT // 2
    level = jax.random.uniform(jax.random.fold_in(key, 22), (RECURRENT_COUNT, REC_KEY), jnp.float32)
    slow_gap = jnp.exp(math.log(1.5e-05) + level * math.log(5e-05 / 1.5e-05))
    fast_gap = jnp.exp(math.log(0.02) + level * math.log(3.0))
    gap = jnp.where(slow[:, None], slow_gap, fast_gap)
    return (1.0 - gap).reshape(KEY_WIDTH).astype(jnp.float32)


def draw_decay_shift(key, part):
    blocks = SEQ // TOK_DEV
    level = jax.random.uniform(jax.random.fold_in(key, 31), (blocks, KEY_WIDTH), jnp.float32)
    rate = jnp.exp(math.log(2.5e-06) + level * math.log(3e-05 / 2.5e-06))
    shift_floor_amount = -jnp.repeat(rate, TOK_DEV, axis=0)
    spots = jax.random.randint(jax.random.fold_in(key, 32), (3,), 0, SEQ)
    leftover_stick = jax.random.uniform(jax.random.fold_in(key, 33), (3, KEY_WIDTH), jnp.float32, 0.2, 0.5)
    stick_fraction = (jnp.arange(SEQ, dtype=jnp.int32)[:, None] == spots[None, :]).astype(jnp.float32)
    segment_tile = jnp.dot(stick_fraction, jnp.log(1.0 - leftover_stick), precision=jax.lax.Precision.HIGHEST)
    return (shift_floor_amount + segment_tile).astype(jnp.float32)


def block_levels(key, extent, cuts, smallest, top_value):
    factor_of, own = 1.0, jax.random.fold_in(key, 6)
    for dim, parts in cuts:
        heights = jnp.exp(jax.random.uniform(jax.random.fold_in(own, dim), (parts,), jnp.float32, smallest / len(cuts), top_value / len(cuts)))
        factor_of = factor_of * jnp.repeat(heights, extent[dim] // parts).reshape([-1 if axis == dim else 1 for axis in range(len(extent))])
    return factor_of


def noise(stream_key, dims, spread, bound, cuts=(), kind=jnp.bfloat16):
    drawn = jax.random.normal(stream_key, dims, jnp.float32) * spread
    if len(cuts) > 0:
        drawn = block_levels(stream_key, dims, cuts, -0.22, 0.18) * drawn
    return jnp.clip(drawn, min=-bound, max=bound).astype(kind)


def setup_inputs(seed: int = 0, part: int = 0) -> dict:
    key_of = jax.random.split(jax.random.key(seed), 15)
    own_keys = jax.random.split(jax.random.fold_in(key_of[14], part), 15)
    return {
        "tokens": noise(own_keys[0], (SEQ, D), 1.0, 6.0, ((0, 4), (1, 4))),
        "norm_gain": jnp.clip(1.0 + 0.18 * jax.random.normal(key_of[1], (D,), jnp.float32), 0.1, 1.9),
        "att_q_weight": noise(key_of[2], (ATT_WIDTH, D), (2 * D ** -0.5), 0.625, ((0, 4), (1, 4))),
        "att_k_weight": noise(key_of[3], (KV_WIDTH, D), D ** -0.5, 0.125, ((0, 4), (1, 4))),
        "att_v_weight": noise(key_of[4], (KV_WIDTH, D), D ** -0.5, 0.125, ((0, 4), (1, 4))),
        "rec_q_weight": noise(key_of[5], (KEY_WIDTH, D), D ** -0.5, 0.125, ((0, 4), (1, 4))),
        "rec_f_weight": noise(key_of[6], (KEY_WIDTH, D), D ** -0.5, 0.125, ((0, 4), (1, 4))),
        "rec_i_weight": noise(key_of[7], (VAL_WIDTH, D), D ** -0.5, 0.125, ((0, 4), (1, 4))),
        "att_out_weight": noise(key_of[8], (ATT_WIDTH, D), (3 * ATT_WIDTH ** -0.5), 1.5, ((0, 4), (1, 4))),
        "rec_out_weight": noise(key_of[9], (VAL_WIDTH, D), VAL_WIDTH ** -0.5, 0.1875, ((0, 4), (1, 4))),
        "score_offset": draw_score_offset(jax.random.fold_in(key_of[14], 71), part),
        "lower_bound": draw_lower_bound(jax.random.fold_in(key_of[14], 71), part),
        "decay_shift": draw_decay_shift(jax.random.fold_in(jax.random.fold_in(key_of[14], part), 71), part),
        "rec_gain": jnp.clip(1.0 + 0.18 * jax.random.normal(key_of[13], (VAL_WIDTH,), jnp.float32), 0.1, 1.9),
    }


EPS = 1e-06
TOP_PRECISION = lax.Precision.HIGHEST

def rounded(values):
    return lax.optimization_barrier(values.astype(jnp.bfloat16))

def block_pass(carry, inputs):
    state_matrix = carry
    query_rows, log_decay, keyed_values, value_rows = inputs
    span = query_rows.shape[0]
    cumulative_log = jnp.cumsum(log_decay, axis=0)
    lower = jnp.arange(span, dtype=jnp.int32)[:, None] >= jnp.arange(span, dtype=jnp.int32)[None, :]
    diff = cumulative_log[:, None] - cumulative_log[None, :]
    decay = jnp.exp(jnp.where(lower[:, :, None, None], diff, -jnp.inf))
    score = jnp.einsum('thk,tshk,shk->ths', query_rows, decay, keyed_values, precision=TOP_PRECISION)
    inner = jnp.einsum('ths,shv->thv', score, value_rows, precision=TOP_PRECISION)
    outer_product = jnp.einsum('ril,ilc->ric', query_rows * jnp.exp(cumulative_log), state_matrix, precision=TOP_PRECISION)
    final_state = cumulative_log[-1]
    state_matrix = state_matrix * jnp.exp(final_state)[:, :, None] + jnp.einsum('iag,iax->agx', keyed_values * jnp.exp(final_state[None] - cumulative_log), value_rows, precision=TOP_PRECISION)
    return (state_matrix, inner + outer_product)

def reference(tokens, norm_gain, att_q_weight, att_k_weight, att_v_weight, rec_q_weight, rec_f_weight, rec_i_weight, att_out_weight, rec_out_weight, score_offset, lower_bound, decay_shift, rec_gain):
    raw = tokens.astype(jnp.float32)
    scaled = (raw * norm_gain[None, :]).astype(jnp.bfloat16)
    inv_rms = lax.rsqrt(lax.optimization_barrier(jnp.mean(raw * raw, axis=1)) + EPS)

    def project(weight):
        return rounded(jnp.dot(scaled, weight.T, preferred_element_type=jnp.float32) * inv_rms[:, None])
    att_query = project(att_q_weight)
    att_key = project(att_k_weight)
    att_value = project(att_v_weight)
    rec_query = project(rec_q_weight)
    rec_forget = project(rec_f_weight)
    rec_input = project(rec_i_weight)
    group = ATT_HEADS // KV_HEADS
    qblock = min(128, SEQ)
    queries = att_query.astype(jnp.float32).reshape(SEQ // qblock, qblock, KV_HEADS, group, HEAD)
    keys = att_key.astype(jnp.float32).reshape(SEQ, KV_HEADS, HEAD)
    values = att_value.astype(jnp.float32).reshape(SEQ, KV_HEADS, HEAD)
    offsets = score_offset.reshape(KV_HEADS, group)
    starts = jnp.arange(SEQ // qblock, dtype=jnp.int32) * qblock
    key_pos = jnp.arange(SEQ, dtype=jnp.int32)

    def attend(args):
        query_block, first = args
        score = jnp.einsum('tkgd,skd->tkgs', query_block, keys, precision=TOP_PRECISION) * HEAD ** (-0.5) + offsets[None, :, :, None]
        query_pos = first + jnp.arange(qblock, dtype=jnp.int32)
        visible = (key_pos[None, :] < query_pos[:, None])[:, None, None, :]
        keep = jnp.where(visible, jax.nn.log_sigmoid(-score), 0.0)
        tail = lax.cumsum(keep, axis=3, reverse=True) - keep
        weight = jnp.where(visible, jnp.exp(jax.nn.log_sigmoid(score) + tail), 0.0)
        weight = rounded(weight).astype(jnp.float32)
        return jnp.einsum('tkgs,skd->tkgd', weight, values, precision=TOP_PRECISION)
    att_out = lax.map(attend, (queries, starts)).reshape(SEQ, ATT_WIDTH).astype(jnp.bfloat16)
    logit = rec_forget.astype(jnp.float32)
    gap = 1.0 - lower_bound
    log_decay = jnp.log(lower_bound + gap * jax.nn.sigmoid(logit)) + decay_shift
    keyed_values = gap * jax.nn.sigmoid(-logit)
    rec_q = jax.nn.silu(rec_query.astype(jnp.float32))
    blocks = SEQ // SPAN

    def split(array, depth):
        return array.reshape(blocks, SPAN, RECURRENT_COUNT, depth)
    start_state = jnp.zeros((RECURRENT_COUNT, REC_KEY, REC_VAL), jnp.float32)
    _, rec_raw = lax.scan(block_pass, start_state, (split(rec_q, REC_KEY), split(log_decay, REC_KEY), split(keyed_values, REC_KEY), split(rec_input.astype(jnp.float32), REC_VAL)))
    rec_raw = rec_raw.reshape(SEQ, RECURRENT_COUNT, REC_VAL)
    rescaled_input = rec_raw * lax.rsqrt(lax.optimization_barrier(jnp.mean(rec_raw * rec_raw, axis=2, keepdims=True)) + EPS) * rec_gain.reshape(RECURRENT_COUNT, REC_VAL)
    rec_out = rescaled_input.reshape(SEQ, VAL_WIDTH).astype(jnp.bfloat16)
    att_cols = ATT_WIDTH // N_TP
    rec_cols = VAL_WIDTH // N_TP
    total = jnp.zeros((SEQ, D), jnp.float32)
    for group_index in range(N_TP):
        att_part = att_out[:, group_index * att_cols:(group_index + 1) * att_cols]
        rec_part = rec_out[:, group_index * rec_cols:(group_index + 1) * rec_cols]
        partial_value = jnp.dot(att_part, att_out_weight[group_index * att_cols:(group_index + 1) * att_cols], preferred_element_type=jnp.float32)
        partial_value = partial_value + jnp.dot(rec_part, rec_out_weight[group_index * rec_cols:(group_index + 1) * rec_cols], preferred_element_type=jnp.float32)
        total = total + rounded(partial_value).astype(jnp.float32)
    return total.astype(jnp.bfloat16)
```

```python
import functools

import jax
import jax.numpy as jnp
from jax import lax
from jax.experimental import pallas as pl
from jax.experimental.pallas import tpu as pltpu
from jax.sharding import PartitionSpec as P

HEAD = 64
REC_KEY = 128
REC_VAL = 128
SPAN = 64


EPS = 1e-06
TOP_PRECISION = lax.Precision.HIGHEST


def entering(x, axis, combine, identity):
    count, here = (lax.axis_size(axis), lax.axis_index(axis))
    everything = jax.tree.map(
        lambda part, kind: lax.all_gather(part.astype(kind), axis), x, (jnp.bfloat16, jnp.bfloat16)
    )
    start = jax.tree.map(
        lambda part, zero: jnp.broadcast_to(jnp.asarray(zero, part.dtype), part.shape), x, identity
    )

    def entering_turn(k, before):
        reached = k < here
        new = combine(
            before, jax.tree.map(lambda part, own: part[k].astype(own.dtype), everything, x)
        )
        return jax.tree.map(lambda a, b: jnp.where(reached, a, b), new, before)

    return lax.fori_loop(0, count, entering_turn, start)


def make_fold(norm_gain, weights, carry, piece):
    elementwise_sq, totals = carry
    raw = piece.astype(jnp.float32)
    scaled = (raw * norm_gain[None, :]).astype(jnp.bfloat16)
    elementwise_sq = jnp.sum(raw * raw, axis=1)
    updated = []
    for total, weight in zip(totals, weights):
        updated.append(
            lax.dot_general(
                scaled, weight, (((1,), (1,)), ((), ())), preferred_element_type=jnp.float32
            )
        )
    return (elementwise_sq, tuple(updated))


def project_all(tokens, norm_gain, weights):
    rows = tokens.shape[0]
    width = weights[0].shape[1]
    start_carry = (
        jnp.zeros((rows,), jnp.float32),
        tuple((jnp.zeros((rows, weight.shape[0]), jnp.float32) for weight in weights)),
    )
    elementwise_sq, totals = make_fold(
        norm_gain, weights, start_carry, lax.all_gather(tokens, "tp", axis=1, tiled=True)
    )
    inv_rms = lax.rsqrt(elementwise_sq / width + EPS)
    return tuple((total * inv_rms[:, None] for total in totals))


def attention(att_query, key_value, score_offset):
    rows = att_query.shape[0]
    gathered = lax.all_gather(key_value, "sp", axis=0, tiled=True)
    seq = gathered.shape[0]
    kv_heads = key_value.shape[1] // (2 * HEAD)
    q_heads = att_query.shape[1] // HEAD
    group = q_heads // kv_heads
    kv_width = kv_heads * HEAD
    queries = att_query.reshape(rows, kv_heads, group, HEAD)
    offsets = score_offset.reshape(kv_heads, group)
    kblock = min(1024, seq)
    first_row = lax.axis_index("sp") * rows
    query_pos = first_row + jnp.arange(rows, dtype=jnp.int32)
    count = (first_row + rows - 1) // kblock + 1

    def attention_turn(step, carry):
        summed, run = carry
        block_start = (count - 1 - step) * kblock
        block = lax.dynamic_slice_in_dim(gathered, block_start, kblock, 0)
        keys = block[:, :kv_width].reshape(kblock, kv_heads, HEAD)
        values = block[:, kv_width:].reshape(kblock, kv_heads, HEAD)
        score = (
            jnp.einsum("tkgd,skd->tkgs", queries, keys, preferred_element_type=jnp.float32)
            * HEAD ** (-0.5)
            + offsets[None, :, :, None]
        )
        key_pos = block_start + jnp.arange(kblock, dtype=jnp.int32)
        visible = (key_pos[None, :] < query_pos[:, None])[:, None, None, :]
        keep = jnp.where(visible, jax.nn.log_sigmoid(-score), 0.0)
        tail = lax.cumsum(keep, axis=3, reverse=True) - keep
        weight = jnp.where(
            visible, jnp.exp(jax.nn.log_sigmoid(score) + tail + run[..., None]), 0.0
        ).astype(jnp.bfloat16)
        summed = summed + jnp.einsum(
            "tkgs,skd->tkgd", weight, values, preferred_element_type=jnp.float32
        )
        return (summed, run + jnp.sum(keep, axis=3))

    start_carry = (
        jnp.zeros((rows, kv_heads, group, HEAD), jnp.float32),
        jnp.zeros((rows, kv_heads, group), jnp.float32),
    )
    summed, _ = lax.fori_loop(0, count, attention_turn, start_carry)
    return summed.reshape(rows, q_heads * HEAD).astype(jnp.bfloat16)


def block_pass(carry, inputs):
    state_matrix, prefix = carry
    query_rows, log_decay, keyed_values, value_rows = inputs
    span = query_rows.shape[0]
    cumulative_log = jnp.cumsum(log_decay, axis=0)
    lower = jnp.arange(span, dtype=jnp.int32)[:, None] >= jnp.arange(span, dtype=jnp.int32)[None, :]
    diff = cumulative_log[:, None] - cumulative_log[None, :]
    decay = jnp.exp(jnp.where(lower[:, :, None, None], diff, -jnp.inf))
    score = jnp.einsum(
        "thk,tshk,shk->ths", query_rows, decay, keyed_values, precision=TOP_PRECISION
    )
    inner = jnp.einsum("ths,shv->thv", score, value_rows, precision=TOP_PRECISION)
    outer_product = jnp.einsum(
        "ril,ilc->ric", query_rows * jnp.exp(cumulative_log), state_matrix, precision=TOP_PRECISION
    )
    final_state = cumulative_log[-1]
    state_matrix = state_matrix * jnp.exp(final_state)[:, :, None] + jnp.einsum(
        "iag,iax->agx",
        keyed_values * jnp.exp(final_state[None] - cumulative_log),
        value_rows,
        precision=TOP_PRECISION,
    )
    reach_limit = query_rows * jnp.exp(cumulative_log + prefix[None])
    return ((state_matrix, prefix + final_state), (inner + outer_product, reach_limit))


def chain(earlier, later):
    return (earlier[0] * later[0], earlier[1] * later[0][:, :, None] + later[1])


def recurrence(rec_query, rec_forget, rec_input, lower_bound, decay_shift, rec_gain):
    rows = rec_query.shape[0]
    heads = rec_gain.shape[0] // REC_VAL
    logit = rec_forget.astype(jnp.float32)
    gap = 1.0 - lower_bound
    log_decay = jnp.log(lower_bound + gap * jax.nn.sigmoid(logit)) + decay_shift
    keyed_values = gap * jax.nn.sigmoid(-logit)
    query_rows = jax.nn.silu(rec_query.astype(jnp.float32))
    blocks = rows // SPAN

    def split(array, depth):
        return array.reshape(blocks, SPAN, heads, depth)

    start_carry = (
        jnp.zeros((heads, REC_KEY, REC_VAL), jnp.float32),
        jnp.zeros((heads, REC_KEY), jnp.float32),
    )
    (state_matrix, total), (local, reach_limit) = lax.scan(
        block_pass,
        start_carry,
        (
            split(query_rows, REC_KEY),
            split(log_decay, REC_KEY),
            split(keyed_values, REC_KEY),
            split(rec_input.astype(jnp.float32), REC_VAL),
        ),
    )
    identity = (
        jnp.ones((heads, REC_KEY), jnp.float32),
        jnp.zeros((heads, REC_KEY, REC_VAL), jnp.float32),
    )
    incoming_state = entering((jnp.exp(total), state_matrix), "sp", chain, identity)
    running_memory = jnp.einsum(
        "lida,dao->lido", reach_limit, incoming_state[1], precision=TOP_PRECISION
    )
    rec_raw = (local + running_memory).reshape(rows, heads, REC_VAL)
    rescaled_input = (
        rec_raw
        * lax.rsqrt(jnp.mean(rec_raw * rec_raw, axis=2, keepdims=True) + EPS)
        * rec_gain.reshape(heads, REC_VAL)
    )
    return rescaled_input.reshape(rows, heads * REC_VAL).astype(jnp.bfloat16)


def gathered_plan(
    tokens,
    norm_gain,
    att_q_weight,
    att_k_weight,
    att_v_weight,
    rec_q_weight,
    rec_f_weight,
    rec_i_weight,
    att_out_weight,
    rec_out_weight,
    score_offset,
    lower_bound,
    decay_shift,
    rec_gain,
):
    inputs = (
        lax.all_gather(att_q_weight, "sp", axis=1, tiled=True),
        lax.all_gather(att_k_weight, "sp", axis=1, tiled=True),
        lax.all_gather(att_v_weight, "sp", axis=1, tiled=True),
        lax.all_gather(rec_q_weight, "sp", axis=1, tiled=True),
        lax.all_gather(rec_f_weight, "sp", axis=1, tiled=True),
        lax.all_gather(rec_i_weight, "sp", axis=1, tiled=True),
    )
    projected = project_all(tokens, norm_gain, inputs)
    att_query = projected[0].astype(jnp.bfloat16)
    key_value = jnp.concatenate(projected[1:3], axis=1).astype(jnp.bfloat16)
    rec_query = projected[3].astype(jnp.bfloat16)
    rec_forget = projected[4].astype(jnp.bfloat16)
    rec_input = projected[5].astype(jnp.bfloat16)
    att_out = attention(att_query, key_value, score_offset)
    rec_out = recurrence(rec_query, rec_forget, rec_input, lower_bound, decay_shift, rec_gain)
    outputs = (
        lax.all_gather(att_out_weight, "sp", axis=1, tiled=True),
        lax.all_gather(rec_out_weight, "sp", axis=1, tiled=True),
    )
    att_rows, rec_rows = outputs
    return lax.psum_scatter(
        (
            jnp.dot(att_out, att_rows, preferred_element_type=jnp.float32)
            + jnp.dot(rec_out, rec_rows, preferred_element_type=jnp.float32)
        ).astype(jnp.bfloat16),
        "tp",
        scatter_dimension=0,
        tiled=True,
    )


MESH = pl.DeviceIdType.MESH
HALVES = 2
STEP = 32


def dot_nt(a, b):
    return lax.dot_general(a, b, (((1,), (1,)), ((), ())), preferred_element_type=jnp.float32)


def dot_tn(a, b):
    return lax.dot_general(a, b, (((0,), (0,)), ((), ())), preferred_element_type=jnp.float32)


def dot_nn(a, b):
    return jnp.dot(a, b, preferred_element_type=jnp.float32)


def remote(src, dst, send_sem, recv_sem, target):
    return pltpu.make_async_remote_copy(
        src_ref=src,
        dst_ref=dst,
        send_sem=send_sem,
        recv_sem=recv_sem,
        device_id=target,
        device_id_type=MESH,
    )


def role_table(count, att_count, rec_count):
    first = rec_count - rec_count // 2
    return (
        [("rec", j) for j in range(first)]
        + [("att", j) for j in range(att_count)]
        + [("rec", j) for j in range(first, rec_count)]
    )


def select_static(index, values):
    result = jnp.int32(0)
    for k, value in enumerate(values):
        result = jnp.where(index == k, jnp.int32(value), result)
    return result


def project_kernel(
    roles, n, nt, width,
    tok_ref, gain_ref, aq_ref, ak_ref, av_ref, rq_ref, rf_ref, ri_ref, shift_ref,
    out_ref, shifts_ref,
    tbuf, squares, scaled, part, send_r, recv_r, send_l, recv_l,
    a_send, a_recv, a_local, b_send, b_recv, d_send, d_recv, d_local, q_send, q_recv,
    rs_sem, rr_sem, ls_sem, lr_sem,
):
    s, t = lax.axis_index("sp"), lax.axis_index("tp")
    rows, feats = tok_ref.shape
    piece = rows // nt
    seq = rows * n

    barrier = pltpu.get_barrier_semaphore()
    for a in range(n):
        for b in range(nt):
            if a or b:
                pl.semaphore_signal(
                    barrier, inc=1,
                    device_id={"sp": lax.rem(s + a, n), "tp": lax.rem(t + b, nt)},
                    device_id_type=MESH,
                )
    pl.semaphore_wait(barrier, n * nt - 1)

    def first_copy(j):
        return remote(
            tok_ref.at[pl.ds(j * piece, piece)], tbuf.at[s, j], a_send.at[j], a_recv.at[s],
            {"sp": t, "tp": j},
        )

    def first_here(j):
        return pltpu.make_async_copy(
            tok_ref.at[pl.ds(j * piece, piece)], tbuf.at[s, j], a_local
        )

    for j in range(nt):
        here = (s == t) & (t == j)
        pl.when(jnp.logical_not(here))(lambda j=j: first_copy(j).start())
        pl.when(here)(lambda j=j: first_here(j).start())

    key = shifts_ref.shape[1]

    def shift_copy(u, j):
        return remote(
            shift_ref.at[:, pl.ds(j * key, key)], shifts_ref.at[pl.ds(s * rows, rows)],
            d_send.at[j], d_recv.at[s], {"sp": u},
        )

    def shift_here(j):
        return pltpu.make_async_copy(
            shift_ref.at[:, pl.ds(j * key, key)], shifts_ref.at[pl.ds(s * rows, rows)], d_local
        )

    recs = [(u, j) for u, (kind, j) in enumerate(roles) if kind == "rec"]
    for u, j in recs:
        pl.when(s != u)(lambda u=u, j=j: shift_copy(u, j).start())
        pl.when(s == u)(lambda j=j: shift_here(j).start())

    def second_copy(k, d):
        return remote(
            tbuf.at[k, t], tbuf.at[k, t], b_send.at[k, d], b_recv.at[k, d],
            {"tp": lax.rem(t + d, nt)},
        )

    for k in range(n):
        here = (s == k) & (t == k)

        def arrived(k=k):
            remote(
                tok_ref.at[pl.ds(0, piece)], tbuf.at[k, t], a_send.at[0], a_recv.at[k],
                {"sp": t, "tp": t},
            ).wait_recv()

        pl.when(jnp.logical_not(here))(arrived)
        pl.when(here)(lambda k=k: first_here(k).wait())
        for d in range(1, nt):
            second_copy(k, d).start()

    gain = gain_ref[:, pl.ds(pl.multiple_of(s * feats, feats), feats)]
    for k in range(n):
        for d in range(1, nt):
            second_copy(k, d).wait_recv()
        raw = tbuf[k].reshape(rows, feats).astype(jnp.float32)
        scaled[pl.ds(k * rows, rows)] = (raw * gain).astype(jnp.bfloat16)
        total = jnp.sum(raw * raw, axis=1, keepdims=True)
        flat = jnp.transpose(jnp.broadcast_to(total, (rows, 128)))
        squares[s, :, pl.ds(k * rows, rows)] = flat[:8]

    def square_copy(a):
        return remote(
            squares.at[s], squares.at[s], q_send.at[a], q_recv.at[a], {"sp": lax.rem(s + a, n)}
        )

    for a in range(1, n):
        square_copy(a).start()

    half = seq // HALVES

    def right_copy(u, h):
        at = (u, pl.ds(h * half, half), pl.ds(0, width[u]))
        return remote(
            send_r.at[at], recv_r.at[at], rs_sem.at[u, h], rr_sem.at[u, h],
            {"sp": jnp.minimum(s + 1, n - 1)},
        )

    def left_copy(u, h):
        at = (u, pl.ds(h * half, half), pl.ds(0, width[u]))
        return remote(
            send_l.at[at], recv_l.at[at], ls_sem.at[u, h], lr_sem.at[u, h],
            {"sp": jnp.maximum(s - 1, 0)},
        )

    order = []
    for i in range(n // 2):
        order += [n - 1 - i, i]
    for u in order:
        kind, j = roles[u]
        if kind == "att":
            group = aq_ref.shape[0] // ak_ref.shape[0]
            pieces = [
                aq_ref[pl.ds(j * group * HEAD, group * HEAD)],
                ak_ref[pl.ds(j * HEAD, HEAD)],
                av_ref[pl.ds(j * HEAD, HEAD)],
            ]
        else:
            pieces = [
                rq_ref[pl.ds(j * REC_KEY, REC_KEY)],
                rf_ref[pl.ds(j * REC_KEY, REC_KEY)],
                ri_ref[pl.ds(j * REC_VAL, REC_VAL)],
            ]
        weight = jnp.concatenate(pieces, axis=0)
        for h in range(HALVES):
            at = (u, pl.ds(h * half, half), pl.ds(0, width[u]))
            product = dot_nt(scaled[pl.ds(h * half, half)], weight)
            part[at] = product
            if u > 0:
                @pl.when(s == 0)
                def _():
                    send_r[at] = product.astype(jnp.bfloat16)
                    right_copy(u, h).start()
            if u < n - 1:
                @pl.when(s == n - 1)
                def _():
                    send_l[at] = product.astype(jnp.bfloat16)
                    left_copy(u, h).start()

    for i in range(n - 1):
        for h in range(HALVES):
            u = n - 1 - i
            at = (u, pl.ds(h * half, half), pl.ds(0, width[u]))

            @pl.when((s > 0) & (s < u))
            def _():
                right_copy(u, h).wait_recv()
                send_r[at] = (part[at] + recv_r[at].astype(jnp.float32)).astype(jnp.bfloat16)
                right_copy(u, h).start()

            v = i
            bt = (v, pl.ds(h * half, half), pl.ds(0, width[v]))

            @pl.when((s < n - 1) & (s > v))
            def _():
                left_copy(v, h).wait_recv()
                send_l[bt] = (part[bt] + recv_l[bt].astype(jnp.float32)).astype(jnp.bfloat16)
                left_copy(v, h).start()

    for a in range(1, n):
        square_copy(a).wait_recv()
    total = squares[0, :1]
    for k in range(1, n):
        total = total + squares[k, :1]
    inv_rms = lax.rsqrt(total / gain_ref.shape[1] + EPS)
    inv_rms = jnp.transpose(jnp.broadcast_to(inv_rms, (128, seq)))
    for u in range(n):
        @pl.when(s == u)
        def _():
            for h in range(HALVES):
                at = (u, pl.ds(h * half, half), pl.ds(0, width[u]))
                result = part[at]
                if u > 0:
                    right_copy(u, h).wait_recv()
                    result = result + recv_r[at].astype(jnp.float32)
                if u < n - 1:
                    left_copy(u, h).wait_recv()
                    result = result + recv_l[at].astype(jnp.float32)
                factor = inv_rms[h * half:(h + 1) * half]
                for c in range(width[u] // 128):
                    out_ref[pl.ds(h * half, half), pl.ds(c * 128, 128)] = (
                        result[:, c * 128:(c + 1) * 128] * factor
                    ).astype(jnp.bfloat16)

    for j in range(nt):
        here = (s == t) & (t == j)
        pl.when(jnp.logical_not(here))(lambda j=j: first_copy(j).wait_send())
    for u, j in recs:
        pl.when(s != u)(lambda u=u, j=j: shift_copy(u, j).wait_send())

        @pl.when(s == u)
        def _():
            shift_here(j).wait()
            for k in range(n):
                if k != u:
                    remote(
                        shift_ref.at[:, pl.ds(j * key, key)], shifts_ref.at[pl.ds(k * rows, rows)],
                        d_send.at[j], d_recv.at[k], {"sp": k},
                    ).wait_recv()
    for k in range(n):
        for d in range(1, nt):
            second_copy(k, d).wait_send()
    for a in range(1, n):
        square_copy(a).wait_send()
    for u in range(n):
        for h in range(HALVES):
            if u > 0:
                pl.when(s < u)(lambda u=u, h=h: right_copy(u, h).wait_send())
            if u < n - 1:
                pl.when(s > u)(lambda u=u, h=h: left_copy(u, h).wait_send())


def stick_mixer(j, group, x_ref, offset_ref, out_ref):
    seq = x_ref.shape[0]
    block = min(128, seq)
    low = lax.broadcasted_iota(jnp.int32, (block, block), 0)
    high = lax.broadcasted_iota(jnp.int32, (block, block), 1)
    later = (low > high).astype(jnp.bfloat16)
    visible = jnp.concatenate([high < low] * group, axis=0)
    offset = jnp.concatenate(
        [jnp.full((block, block), offset_ref[j * group + g], jnp.float32) for g in range(group)],
        axis=0,
    )
    keys = x_ref[:, group * HEAD:(group + 1) * HEAD]
    values = x_ref[:, (group + 1) * HEAD:(group + 2) * HEAD]
    for q in range(seq // block):
        queries = x_ref[q * block:(q + 1) * block, :group * HEAD]
        queries = jnp.concatenate(
            [queries[:, g * HEAD:(g + 1) * HEAD] for g in range(group)], axis=0
        )
        run = jnp.zeros((group * block, 1), jnp.float32)
        summed = jnp.zeros((group * block, HEAD), jnp.float32)
        for c in range(q, -1, -1):
            at = slice(c * block, (c + 1) * block)
            score = dot_nt(queries, keys[at]) * HEAD ** (-0.5) + offset
            keep = -(jnp.maximum(score, 0.0) + jnp.log1p(jnp.exp(-jnp.abs(score))))
            gate = score + keep
            if c == q:
                keep = jnp.where(visible, keep, 0.0)
            top = keep.astype(jnp.bfloat16)
            rest = (keep - top.astype(jnp.float32)).astype(jnp.bfloat16)
            tail = dot_nn(top, later) + dot_nn(rest, later)
            weight = jnp.exp(gate + tail + run)
            if c == q:
                weight = jnp.where(visible, weight, 0.0)
            summed = summed + dot_nn(weight.astype(jnp.bfloat16), values[at])
            run = run + jnp.sum(keep, axis=1, keepdims=True)
        out_ref[q * block:(q + 1) * block] = jnp.concatenate(
            [summed[g * block:(g + 1) * block] for g in range(group)], axis=1
        ).astype(jnp.bfloat16)


def state_mixer(j, x_ref, bound_ref, shift_ref, gain_ref, out_ref):
    seq = x_ref.shape[0]
    block = min(128, seq)
    bound = bound_ref[:, pl.ds(pl.multiple_of(j * REC_KEY, REC_KEY), REC_KEY)]
    gain = gain_ref[:, pl.ds(pl.multiple_of(j * REC_VAL, REC_VAL), REC_VAL)]
    gap = 1.0 - bound
    low = lax.broadcasted_iota(jnp.int32, (block, block), 0)
    high = lax.broadcasted_iota(jnp.int32, (block, block), 1)
    upto = ((high <= low) & (high // STEP == low // STEP)).astype(jnp.float32)
    lower = (
        lax.broadcasted_iota(jnp.int32, (STEP, STEP), 0)
        >= lax.broadcasted_iota(jnp.int32, (STEP, STEP), 1)
    )
    state = jnp.zeros((REC_VAL, REC_KEY), jnp.float32)
    for b in range(seq // block):
        at = slice(b * block, (b + 1) * block)
        logit = x_ref[at, REC_KEY:2 * REC_KEY].astype(jnp.float32)
        query = x_ref[at, :REC_KEY].astype(jnp.float32)
        value = x_ref[at, 2 * REC_KEY:2 * REC_KEY + REC_VAL]
        log_decay = jnp.log(bound + gap * jax.nn.sigmoid(logit)) + shift_ref[at]
        keyed = gap * jax.nn.sigmoid(-logit)
        query = query * jax.nn.sigmoid(query)
        running = jnp.dot(
            upto, log_decay, precision=TOP_PRECISION, preferred_element_type=jnp.float32
        )
        for i in range(block // STEP):
            it = slice(i * STEP, (i + 1) * STEP)
            cumulative, q, k, v = running[it], query[it], keyed[it], value[it]
            middle = cumulative[STEP // 2 - 1:STEP // 2]
            last = cumulative[STEP - 1:STEP]
            score = dot_nt(
                (q * jnp.exp(cumulative - middle)).astype(jnp.bfloat16),
                (k * jnp.exp(middle - cumulative)).astype(jnp.bfloat16),
            )
            score = jnp.where(lower, score, 0.0).astype(jnp.bfloat16)
            raw = dot_nn(score, v) + dot_nt(
                (q * jnp.exp(cumulative)).astype(jnp.bfloat16), state.astype(jnp.bfloat16)
            )
            state = state * jnp.exp(last) + dot_tn(
                v, (k * jnp.exp(last - cumulative)).astype(jnp.bfloat16)
            )
            scale = lax.rsqrt(jnp.mean(raw * raw, axis=1, keepdims=True) + EPS)
            out_ref[b * block + i * STEP:b * block + (i + 1) * STEP] = (
                raw * scale * gain
            ).astype(jnp.bfloat16)


def mix_kernel(roles, group, x_ref, offset_ref, bound_ref, shift_ref, gain_ref, out_ref):
    s = lax.axis_index("sp")
    j = select_static(s, [index for _, index in roles])
    is_rec = select_static(s, [int(kind == "rec") for kind, _ in roles])

    @pl.when(is_rec == 0)
    def _():
        stick_mixer(j, group, x_ref, offset_ref, out_ref)

    @pl.when(is_rec == 1)
    def _():
        state_mixer(j, x_ref, bound_ref, shift_ref, gain_ref, out_ref)


def output_kernel(
    roles, n, nt,
    x_ref, wa_ref, wr_ref, out_ref,
    heads, part, landed, mixed,
    e_send, e_recv, e_local, f_send, f_recv, g_send, g_recv, g_local,
):
    s, t = lax.axis_index("sp"), lax.axis_index("tp")
    seq, wide = x_ref.shape
    piece = seq // (n * nt)
    cols = wa_ref.shape[1]

    barrier = pltpu.get_barrier_semaphore()
    for a in range(1, n):
        pl.semaphore_signal(
            barrier, inc=1, device_id={"sp": lax.rem(s + a, n)}, device_id_type=MESH
        )
    for b in range(1, nt):
        pl.semaphore_signal(
            barrier, inc=1, device_id={"tp": lax.rem(t + b, nt)}, device_id_type=MESH
        )
    pl.semaphore_wait(barrier, n + nt - 2)

    def head_copy(a):
        return remote(
            x_ref, heads.at[s], e_send.at[a], e_recv.at[a], {"sp": lax.rem(s + a, n)}
        )

    own = pltpu.make_async_copy(x_ref, heads.at[s], e_local)
    own.start()
    for a in range(1, n):
        head_copy(a).start()
    own.wait()
    for a in range(1, n):
        head_copy(a).wait_recv()

    total = None
    for u, (kind, j) in enumerate(roles):
        ref = wa_ref if kind == "att" else wr_ref
        term = dot_nn(heads[u], ref[pl.ds(j * wide, wide)])
        total = term if total is None else total + term
    part[...] = total.astype(jnp.bfloat16).reshape(n, nt, piece, cols)

    def share_copy(b):
        to = lax.rem(t + b, nt)
        return remote(
            part.at[:, to], landed.at[b], f_send.at[b], f_recv.at[b], {"tp": to}
        )

    for b in range(1, nt):
        share_copy(b).start()
    result = part[:, t].astype(jnp.float32)
    for b in range(1, nt):
        share_copy(b).wait_recv()
        result = result + landed[b].astype(jnp.float32)
    mixed[...] = result.astype(jnp.bfloat16)

    place = out_ref.at[:, pl.ds(pl.multiple_of(s * cols, cols), cols)]

    def final_copy(a):
        to = lax.rem(s + a, n)
        return remote(mixed.at[to], place, g_send.at[a], g_recv.at[a], {"sp": to})

    here = pltpu.make_async_copy(mixed.at[s], place, g_local)
    for a in range(1, n):
        final_copy(a).start()
    here.start()
    here.wait()
    for a in range(1, n):
        remote(
            mixed.at[s],
            out_ref.at[:, pl.ds(pl.multiple_of(lax.rem(s + n - a, n) * cols, cols), cols)],
            g_send.at[a], g_recv.at[a], {"sp": lax.rem(s + a, n)},
        ).wait_recv()
    for a in range(1, n):
        head_copy(a).wait_send()
        final_copy(a).wait_send()
    for b in range(1, nt):
        share_copy(b).wait_send()


def stationary_fits(args):
    n, nt = lax.axis_size("sp"), lax.axis_size("tp")
    tokens, att_q, att_k, rec_q, rec_i = args[0], args[2], args[3], args[5], args[7]
    rows, feats = tokens.shape
    att_count, rec_count = att_k.shape[0] // HEAD, rec_i.shape[0] // REC_VAL
    group = att_q.shape[0] // att_k.shape[0]
    return (
        n == nt
        and n % 2 == 0
        and att_count + rec_count == n
        and group * HEAD == REC_VAL
        and feats == att_q.shape[1]
        and rows % 128 == 0
        and rows * n <= 1024
    )


def stationary(
    tokens, norm_gain, att_q_weight, att_k_weight, att_v_weight, rec_q_weight, rec_f_weight,
    rec_i_weight, att_out_weight, rec_out_weight, score_offset, lower_bound, decay_shift, rec_gain,
):
    n, nt = lax.axis_size("sp"), lax.axis_size("tp")
    rows, feats = tokens.shape
    seq = rows * n
    cols = att_out_weight.shape[1]
    group = att_q_weight.shape[0] // att_k_weight.shape[0]
    roles = role_table(n, att_k_weight.shape[0] // HEAD, rec_i_weight.shape[0] // REC_VAL)
    width = [(group + 2) * HEAD if kind == "att" else 2 * REC_KEY + REC_VAL for kind, _ in roles]
    widest = max(width)
    bf16, f32 = jnp.bfloat16, jnp.float32
    dma = pltpu.SemaphoreType.DMA
    vmem = pl.BlockSpec(memory_space=pltpu.VMEM)
    smem = pl.BlockSpec(memory_space=pltpu.SMEM)
    projected, shifts = pl.pallas_call(
        functools.partial(project_kernel, roles, n, nt, width),
        out_shape=(
            jax.ShapeDtypeStruct((seq, widest), bf16),
            jax.ShapeDtypeStruct((seq, REC_KEY), f32),
        ),
        in_specs=[vmem] * 9,
        out_specs=(vmem, vmem),
        scratch_shapes=[
            pltpu.VMEM((n, nt, rows // nt, feats), bf16),
            pltpu.VMEM((n, 8, seq), f32),
            pltpu.VMEM((seq, feats), bf16),
            pltpu.VMEM((n, seq, widest), f32),
            pltpu.VMEM((n, seq, widest), bf16),
            pltpu.VMEM((n, seq, widest), bf16),
            pltpu.VMEM((n, seq, widest), bf16),
            pltpu.VMEM((n, seq, widest), bf16),
            dma((nt,)), dma((n,)), dma, dma((n, nt)), dma((n, nt)),
            dma((n,)), dma((n,)), dma, dma((n,)), dma((n,)),
            dma((n, HALVES)), dma((n, HALVES)), dma((n, HALVES)), dma((n, HALVES)),
        ],
        compiler_params=pltpu.CompilerParams(collective_id=0, has_side_effects=True),
        name="project",
    )(
        tokens, norm_gain.reshape(1, -1), att_q_weight, att_k_weight, att_v_weight,
        rec_q_weight, rec_f_weight, rec_i_weight, decay_shift,
    )
    heads = pl.pallas_call(
        functools.partial(mix_kernel, roles, group),
        out_shape=jax.ShapeDtypeStruct((seq, REC_VAL), bf16),
        in_specs=[vmem, smem, vmem, vmem, vmem],
        out_specs=vmem,
        name="mix",
    )(projected, score_offset, lower_bound.reshape(1, -1), shifts, rec_gain.reshape(1, -1))
    return pl.pallas_call(
        functools.partial(output_kernel, roles, n, nt),
        out_shape=jax.ShapeDtypeStruct((seq // (n * nt), cols * n), bf16),
        in_specs=[vmem] * 3,
        out_specs=vmem,
        scratch_shapes=[
            pltpu.VMEM((n, seq, REC_VAL), bf16),
            pltpu.VMEM((n, nt, seq // (n * nt), cols), bf16),
            pltpu.VMEM((nt, n, seq // (n * nt), cols), bf16),
            pltpu.VMEM((n, seq // (n * nt), cols), bf16),
            dma((n,)), dma((n,)), dma, dma((nt,)), dma((nt,)), dma((n,)), dma((n,)), dma,
        ],
        compiler_params=pltpu.CompilerParams(collective_id=1, has_side_effects=True),
        name="output",
    )(heads, att_out_weight, rec_out_weight)


def on_device(*args):
    if stationary_fits(args):
        return stationary(*args)
    return gathered_plan(*args)


def solution(mesh):
    in_specs = (
        P(("grp", "sp"), "tp"),
        P(),
        P("tp", "sp"),
        P("tp", "sp"),
        P("tp", "sp"),
        P("tp", "sp"),
        P("tp", "sp"),
        P("tp", "sp"),
        P("tp", "sp"),
        P("tp", "sp"),
        P("tp"),
        P("tp"),
        P(("grp", "sp"), "tp"),
        P("tp"),
    )
    out_specs = P(("grp", "sp", "tp"), None)
    return jax.shard_map(
        on_device, mesh=mesh, in_specs=in_specs, out_specs=out_specs, check_vma=False
    )
```

```python
import functools

import jax
import jax.numpy as jnp
from jax import lax
from jax.experimental import pallas as pl
from jax.experimental.pallas import tpu as pltpu
from jax.sharding import PartitionSpec as P

HEAD = 64
REC_KEY = 128
REC_VAL = 128
SPAN = 64


EPS = 1e-06
TOP_PRECISION = lax.Precision.HIGHEST


def entering(x, axis, combine, identity):
    count, here = (lax.axis_size(axis), lax.axis_index(axis))
    everything = jax.tree.map(
        lambda part, kind: lax.all_gather(part.astype(kind), axis), x, (jnp.bfloat16, jnp.bfloat16)
    )
    start = jax.tree.map(
        lambda part, zero: jnp.broadcast_to(jnp.asarray(zero, part.dtype), part.shape), x, identity
    )

    def entering_turn(k, before):
        reached = k < here
        new = combine(
            before, jax.tree.map(lambda part, own: part[k].astype(own.dtype), everything, x)
        )
        return jax.tree.map(lambda a, b: jnp.where(reached, a, b), new, before)

    return lax.fori_loop(0, count, entering_turn, start)


def make_fold(norm_gain, weights, carry, piece):
    elementwise_sq, totals = carry
    raw = piece.astype(jnp.float32)
    scaled = (raw * norm_gain[None, :]).astype(jnp.bfloat16)
    elementwise_sq = jnp.sum(raw * raw, axis=1)
    updated = []
    for total, weight in zip(totals, weights):
        updated.append(
            lax.dot_general(
                scaled, weight, (((1,), (1,)), ((), ())), preferred_element_type=jnp.float32
            )
        )
    return (elementwise_sq, tuple(updated))


def project_all(tokens, norm_gain, weights):
    rows = tokens.shape[0]
    width = weights[0].shape[1]
    start_carry = (
        jnp.zeros((rows,), jnp.float32),
        tuple((jnp.zeros((rows, weight.shape[0]), jnp.float32) for weight in weights)),
    )
    elementwise_sq, totals = make_fold(
        norm_gain, weights, start_carry, lax.all_gather(tokens, "tp", axis=1, tiled=True)
    )
    inv_rms = lax.rsqrt(elementwise_sq / width + EPS)
    return tuple((total * inv_rms[:, None] for total in totals))


def attention(att_query, key_value, score_offset):
    rows = att_query.shape[0]
    gathered = lax.all_gather(key_value, "sp", axis=0, tiled=True)
    seq = gathered.shape[0]
    kv_heads = key_value.shape[1] // (2 * HEAD)
    q_heads = att_query.shape[1] // HEAD
    group = q_heads // kv_heads
    kv_width = kv_heads * HEAD
    queries = att_query.reshape(rows, kv_heads, group, HEAD)
    offsets = score_offset.reshape(kv_heads, group)
    kblock = min(1024, seq)
    first_row = lax.axis_index("sp") * rows
    query_pos = first_row + jnp.arange(rows, dtype=jnp.int32)
    count = (first_row + rows - 1) // kblock + 1

    def attention_turn(step, carry):
        summed, run = carry
        block_start = (count - 1 - step) * kblock
        block = lax.dynamic_slice_in_dim(gathered, block_start, kblock, 0)
        keys = block[:, :kv_width].reshape(kblock, kv_heads, HEAD)
        values = block[:, kv_width:].reshape(kblock, kv_heads, HEAD)
        score = (
            jnp.einsum("tkgd,skd->tkgs", queries, keys, preferred_element_type=jnp.float32)
            * HEAD ** (-0.5)
            + offsets[None, :, :, None]
        )
        key_pos = block_start + jnp.arange(kblock, dtype=jnp.int32)
        visible = (key_pos[None, :] < query_pos[:, None])[:, None, None, :]
        keep = jnp.where(visible, jax.nn.log_sigmoid(-score), 0.0)
        tail = lax.cumsum(keep, axis=3, reverse=True) - keep
        weight = jnp.where(
            visible, jnp.exp(jax.nn.log_sigmoid(score) + tail + run[..., None]), 0.0
        ).astype(jnp.bfloat16)
        summed = summed + jnp.einsum(
            "tkgs,skd->tkgd", weight, values, preferred_element_type=jnp.float32
        )
        return (summed, run + jnp.sum(keep, axis=3))

    start_carry = (
        jnp.zeros((rows, kv_heads, group, HEAD), jnp.float32),
        jnp.zeros((rows, kv_heads, group), jnp.float32),
    )
    summed, _ = lax.fori_loop(0, count, attention_turn, start_carry)
    return summed.reshape(rows, q_heads * HEAD).astype(jnp.bfloat16)


def block_pass(carry, inputs):
    state_matrix, prefix = carry
    query_rows, log_decay, keyed_values, value_rows = inputs
    span = query_rows.shape[0]
    cumulative_log = jnp.cumsum(log_decay, axis=0)
    lower = jnp.arange(span, dtype=jnp.int32)[:, None] >= jnp.arange(span, dtype=jnp.int32)[None, :]
    diff = cumulative_log[:, None] - cumulative_log[None, :]
    decay = jnp.exp(jnp.where(lower[:, :, None, None], diff, -jnp.inf))
    score = jnp.einsum(
        "thk,tshk,shk->ths", query_rows, decay, keyed_values, precision=TOP_PRECISION
    )
    inner = jnp.einsum("ths,shv->thv", score, value_rows, precision=TOP_PRECISION)
    outer_product = jnp.einsum(
        "ril,ilc->ric", query_rows * jnp.exp(cumulative_log), state_matrix, precision=TOP_PRECISION
    )
    final_state = cumulative_log[-1]
    state_matrix = state_matrix * jnp.exp(final_state)[:, :, None] + jnp.einsum(
        "iag,iax->agx",
        keyed_values * jnp.exp(final_state[None] - cumulative_log),
        value_rows,
        precision=TOP_PRECISION,
    )
    reach_limit = query_rows * jnp.exp(cumulative_log + prefix[None])
    return ((state_matrix, prefix + final_state), (inner + outer_product, reach_limit))


def chain(earlier, later):
    return (earlier[0] * later[0], earlier[1] * later[0][:, :, None] + later[1])


def recurrence(rec_query, rec_forget, rec_input, lower_bound, decay_shift, rec_gain):
    rows = rec_query.shape[0]
    heads = rec_gain.shape[0] // REC_VAL
    logit = rec_forget.astype(jnp.float32)
    gap = 1.0 - lower_bound
    log_decay = jnp.log(lower_bound + gap * jax.nn.sigmoid(logit)) + decay_shift
    keyed_values = gap * jax.nn.sigmoid(-logit)
    query_rows = jax.nn.silu(rec_query.astype(jnp.float32))
    blocks = rows // SPAN

    def split(array, depth):
        return array.reshape(blocks, SPAN, heads, depth)

    start_carry = (
        jnp.zeros((heads, REC_KEY, REC_VAL), jnp.float32),
        jnp.zeros((heads, REC_KEY), jnp.float32),
    )
    (state_matrix, total), (local, reach_limit) = lax.scan(
        block_pass,
        start_carry,
        (
            split(query_rows, REC_KEY),
            split(log_decay, REC_KEY),
            split(keyed_values, REC_KEY),
            split(rec_input.astype(jnp.float32), REC_VAL),
        ),
    )
    identity = (
        jnp.ones((heads, REC_KEY), jnp.float32),
        jnp.zeros((heads, REC_KEY, REC_VAL), jnp.float32),
    )
    incoming_state = entering((jnp.exp(total), state_matrix), "sp", chain, identity)
    running_memory = jnp.einsum(
        "lida,dao->lido", reach_limit, incoming_state[1], precision=TOP_PRECISION
    )
    rec_raw = (local + running_memory).reshape(rows, heads, REC_VAL)
    rescaled_input = (
        rec_raw
        * lax.rsqrt(jnp.mean(rec_raw * rec_raw, axis=2, keepdims=True) + EPS)
        * rec_gain.reshape(heads, REC_VAL)
    )
    return rescaled_input.reshape(rows, heads * REC_VAL).astype(jnp.bfloat16)


def gathered_plan(
    tokens,
    norm_gain,
    att_q_weight,
    att_k_weight,
    att_v_weight,
    rec_q_weight,
    rec_f_weight,
    rec_i_weight,
    att_out_weight,
    rec_out_weight,
    score_offset,
    lower_bound,
    decay_shift,
    rec_gain,
):
    inputs = (
        lax.all_gather(att_q_weight, "sp", axis=1, tiled=True),
        lax.all_gather(att_k_weight, "sp", axis=1, tiled=True),
        lax.all_gather(att_v_weight, "sp", axis=1, tiled=True),
        lax.all_gather(rec_q_weight, "sp", axis=1, tiled=True),
        lax.all_gather(rec_f_weight, "sp", axis=1, tiled=True),
        lax.all_gather(rec_i_weight, "sp", axis=1, tiled=True),
    )
    projected = project_all(tokens, norm_gain, inputs)
    att_query = projected[0].astype(jnp.bfloat16)
    key_value = jnp.concatenate(projected[1:3], axis=1).astype(jnp.bfloat16)
    rec_query = projected[3].astype(jnp.bfloat16)
    rec_forget = projected[4].astype(jnp.bfloat16)
    rec_input = projected[5].astype(jnp.bfloat16)
    att_out = attention(att_query, key_value, score_offset)
    rec_out = recurrence(rec_query, rec_forget, rec_input, lower_bound, decay_shift, rec_gain)
    outputs = (
        lax.all_gather(att_out_weight, "sp", axis=1, tiled=True),
        lax.all_gather(rec_out_weight, "sp", axis=1, tiled=True),
    )
    att_rows, rec_rows = outputs
    return lax.psum_scatter(
        (
            jnp.dot(att_out, att_rows, preferred_element_type=jnp.float32)
            + jnp.dot(rec_out, rec_rows, preferred_element_type=jnp.float32)
        ).astype(jnp.bfloat16),
        "tp",
        scatter_dimension=0,
        tiled=True,
    )


MESH = pl.DeviceIdType.MESH
STEP = 32


def dot_nt(a, b):
    return lax.dot_general(a, b, (((1,), (1,)), ((), ())), preferred_element_type=jnp.float32)


def dot_tn(a, b):
    return lax.dot_general(a, b, (((0,), (0,)), ((), ())), preferred_element_type=jnp.float32)


def dot_nn(a, b):
    return jnp.dot(a, b, preferred_element_type=jnp.float32)


def remote(src, dst, send_sem, recv_sem, target):
    return pltpu.make_async_remote_copy(
        src_ref=src,
        dst_ref=dst,
        send_sem=send_sem,
        recv_sem=recv_sem,
        device_id=target,
        device_id_type=MESH,
    )


SUB = 64


def stick_block(q, j, group, x, offset_ref):
    block = 128
    low = lax.broadcasted_iota(jnp.int32, (block, block), 0)
    high = lax.broadcasted_iota(jnp.int32, (block, block), 1)
    later = (low > high).astype(jnp.bfloat16)
    visible = jnp.concatenate([high < low] * group, axis=0)
    offset = jnp.concatenate(
        [jnp.full((block, block), offset_ref[j * group + g], jnp.float32) for g in range(group)],
        axis=0,
    )
    queries = x[q * block:(q + 1) * block, :group * HEAD]
    queries = jnp.concatenate([queries[:, g * HEAD:(g + 1) * HEAD] for g in range(group)], axis=0)
    run = jnp.zeros((group * block, 1), jnp.float32)
    summed = jnp.zeros((group * block, HEAD), jnp.float32)
    for c in range(q, -1, -1):
        keys = x[c * block:(c + 1) * block, group * HEAD:(group + 1) * HEAD]
        values = x[c * block:(c + 1) * block, (group + 1) * HEAD:(group + 2) * HEAD]
        score = dot_nt(queries, keys) * HEAD ** (-0.5) + offset
        keep = -(jnp.maximum(score, 0.0) + jnp.log1p(jnp.exp(-jnp.abs(score))))
        gate = score + keep
        if c == q:
            keep = jnp.where(visible, keep, 0.0)
        top = keep.astype(jnp.bfloat16)
        rest = (keep - top.astype(jnp.float32)).astype(jnp.bfloat16)
        tail = dot_nn(top, later) + dot_nn(rest, later)
        weight = jnp.exp(gate + tail + run)
        if c == q:
            weight = jnp.where(visible, weight, 0.0)
        summed = summed + dot_nn(weight.astype(jnp.bfloat16), values)
        run = run + jnp.sum(keep, axis=1, keepdims=True)
    return jnp.concatenate(
        [summed[g * block:(g + 1) * block] for g in range(group)], axis=1
    ).astype(jnp.bfloat16)


def state_block(b, j, x, first, bound_ref, shift_ref, gain_ref, state_ref):
    block = 128
    bound = bound_ref[:, pl.ds(pl.multiple_of(j * REC_KEY, REC_KEY), REC_KEY)]
    gain = gain_ref[:, pl.ds(pl.multiple_of(j * REC_VAL, REC_VAL), REC_VAL)]
    gap = 1.0 - bound
    low = lax.broadcasted_iota(jnp.int32, (block, block), 0)
    high = lax.broadcasted_iota(jnp.int32, (block, block), 1)
    upto = ((high <= low) & (high // STEP == low // STEP)).astype(jnp.float32)
    lower = (
        lax.broadcasted_iota(jnp.int32, (STEP, STEP), 0)
        >= lax.broadcasted_iota(jnp.int32, (STEP, STEP), 1)
    )
    state = jnp.zeros((REC_VAL, REC_KEY), jnp.float32) if b == 0 else state_ref[...]
    at = slice(b * block, (b + 1) * block)
    query = x[at, first:first + REC_KEY].astype(jnp.float32)
    logit = x[at, first + REC_KEY:first + 2 * REC_KEY].astype(jnp.float32)
    value = x[at, first + 2 * REC_KEY:first + 2 * REC_KEY + REC_VAL]
    log_decay = jnp.log(bound + gap * jax.nn.sigmoid(logit)) + shift_ref[at]
    keyed = gap * jax.nn.sigmoid(-logit)
    query = query * jax.nn.sigmoid(query)
    running = jnp.dot(upto, log_decay, precision=TOP_PRECISION, preferred_element_type=jnp.float32)
    outs = []
    for i in range(block // STEP):
        it = slice(i * STEP, (i + 1) * STEP)
        cumulative, q, k, v = running[it], query[it], keyed[it], value[it]
        middle = cumulative[STEP // 2 - 1:STEP // 2]
        last = cumulative[STEP - 1:STEP]
        score = dot_nt(
            (q * jnp.exp(cumulative - middle)).astype(jnp.bfloat16),
            (k * jnp.exp(middle - cumulative)).astype(jnp.bfloat16),
        )
        score = jnp.where(lower, score, 0.0).astype(jnp.bfloat16)
        raw = dot_nn(score, v) + dot_nt(
            (q * jnp.exp(cumulative)).astype(jnp.bfloat16), state.astype(jnp.bfloat16)
        )
        state = state * jnp.exp(last) + dot_tn(
            v, (k * jnp.exp(last - cumulative)).astype(jnp.bfloat16)
        )
        scale = lax.rsqrt(jnp.mean(raw * raw, axis=1, keepdims=True) + EPS)
        outs.append((raw * scale * gain).astype(jnp.bfloat16))
    state_ref[...] = state
    return jnp.concatenate(outs, axis=0)


def layer_kernel(
    n, nt, group,
    tok_ref, gain_ref, aq_ref, ak_ref, av_ref, rq_ref, rf_ref, ri_ref, shift_ref,
    wa_ref, wr_ref, offset_ref, bound_ref, rec_gain_ref,
    out_ref,
    tbuf, shifts, squares, part, sent, came, x, state, heads, shares, landed, mixed,
    a_send, a_recv, a_local, b_send, b_recv, d_send, d_recv, d_local, q_send, q_recv,
    c_send, c_recv, e_send, e_recv, f_send, f_recv, g_send, g_recv, g_local,
):
    s, t = lax.axis_index("sp"), lax.axis_index("tp")
    rows, feats = tok_ref.shape
    piece = rows // nt
    width = x.shape[1]
    att_width = (group + 2) * HEAD
    wide = group * HEAD
    cols = wa_ref.shape[1]
    subs = rows // SUB
    ends = (0, n - 1)
    at_end = (s == 0) | (s == n - 1)
    e = s // (n - 1)
    f32, bf16 = jnp.float32, jnp.bfloat16

    barrier = pltpu.get_barrier_semaphore()
    for a in range(n):
        for b in range(nt):
            if a or b:
                pl.semaphore_signal(
                    barrier, inc=1,
                    device_id={"sp": lax.rem(s + a, n), "tp": lax.rem(t + b, nt)},
                    device_id_type=MESH,
                )
    pl.semaphore_wait(barrier, n * nt - 1)

    def first_copy(j):
        return remote(
            tok_ref.at[pl.ds(j * piece, piece)], tbuf.at[s, j], a_send.at[j], a_recv.at[s],
            {"sp": t, "tp": j},
        )

    def first_here(j):
        return pltpu.make_async_copy(
            tok_ref.at[pl.ds(j * piece, piece)], tbuf.at[s, j], a_local
        )

    for j in range(nt):
        here = (s == t) & (t == j)
        pl.when(jnp.logical_not(here))(lambda j=j: first_copy(j).start())
        pl.when(here)(lambda j=j: first_here(j).start())

    def shift_copy(i):
        return remote(
            shift_ref.at[:, pl.ds(i * REC_KEY, REC_KEY)], shifts.at[pl.ds(s * rows, rows)],
            d_send.at[i], d_recv.at[s], {"sp": ends[i]},
        )

    def shift_here(i):
        return pltpu.make_async_copy(
            shift_ref.at[:, pl.ds(i * REC_KEY, REC_KEY)], shifts.at[pl.ds(s * rows, rows)], d_local
        )

    for i, u in enumerate(ends):
        pl.when(s != u)(lambda i=i: shift_copy(i).start())
        pl.when(s == u)(lambda i=i: shift_here(i).start())

    def second_copy(k, d):
        return remote(
            tbuf.at[k, t], tbuf.at[k, t], b_send.at[k, d], b_recv.at[k, d],
            {"tp": lax.rem(t + d, nt)},
        )

    def relay(k):
        here = (s == k) & (t == k)

        def arrived():
            remote(
                tok_ref.at[pl.ds(0, piece)], tbuf.at[k, t], a_send.at[0], a_recv.at[k],
                {"sp": t, "tp": t},
            ).wait_recv()

        pl.when(jnp.logical_not(here))(arrived)
        pl.when(here)(lambda: first_here(k).wait())
        for d in range(1, nt):
            second_copy(k, d).start()

    gain = gain_ref[:, pl.ds(pl.multiple_of(s * feats, feats), feats)]

    def square_copy(k, i):
        return remote(
            squares.at[s, k], squares.at[s, k], q_send.at[k, i], q_recv.at[s, k], {"sp": ends[i]}
        )

    def chain_copy(i, c):
        to = jnp.maximum(s - 1, 0) if i == 0 else jnp.minimum(s + 1, n - 1)
        return remote(
            sent.at[i, pl.ds(c * SUB, SUB)], came.at[i, pl.ds(c * SUB, SUB)],
            c_send.at[i, c], c_recv.at[i, c], {"sp": to},
        )

    weights = []
    for i in range(2):
        weights.append(jnp.concatenate(
            [
                aq_ref[pl.ds(i * wide, wide)],
                ak_ref[pl.ds(i * HEAD, HEAD)],
                av_ref[pl.ds(i * HEAD, HEAD)],
                rq_ref[pl.ds(i * REC_KEY, REC_KEY)],
                rf_ref[pl.ds(i * REC_KEY, REC_KEY)],
                ri_ref[pl.ds(i * REC_VAL, REC_VAL)],
            ],
            axis=0,
        ))

    def project(k):
        for d in range(1, nt):
            second_copy(k, d).wait_recv()
        raw = tbuf[k].reshape(rows, feats).astype(f32)
        scaled = (raw * gain).astype(bf16)
        for i in range(2):
            product = dot_nt(scaled, weights[i])
            part[i, pl.ds(k * rows, rows)] = product

            @pl.when(s == ends[1 - i])
            def _():
                for r in range(subs):
                    c = k * subs + r
                    sent[i, pl.ds(c * SUB, SUB)] = product[r * SUB:(r + 1) * SUB].astype(bf16)
                    chain_copy(i, c).start()

        total = jnp.sum(raw * raw, axis=1, keepdims=True)
        flat = jnp.transpose(jnp.broadcast_to(total, (rows, 128)))
        squares[s, k] = flat[:8]
        for i in range(2):
            pl.when(s != ends[i])(lambda i=i: square_copy(k, i).start())

    def forward(k):
        for r in range(subs):
            c = k * subs + r
            for i in (1, 0):
                chain_copy(i, c).wait_recv()
                at = (i, pl.ds(c * SUB, SUB))
                sent[at] = (part[at] + came[at].astype(f32)).astype(bf16)
                chain_copy(i, c).start()

    def head_copy(i, k, to):
        at = (i, pl.ds(k * rows, rows))
        return remote(
            heads.at[at], heads.at[at], e_send.at[k, to], e_recv.at[i, k], {"sp": to}
        )

    def mix(k):
        span = pl.ds(k * rows, rows)
        for i in range(2):
            @pl.when(s == ends[i])
            def _():
                for r in range(subs):
                    chain_copy(i, k * subs + r).wait_recv()
                for v in range(n):
                    if v != ends[i]:
                        remote(
                            squares.at[v, k], squares.at[v, k], q_send.at[k, i], q_recv.at[v, k],
                            {"sp": v},
                        ).wait_recv()
                if k == ends[i]:
                    shift_here(i).wait()
                else:
                    remote(
                        shift_ref.at[:, pl.ds(i * REC_KEY, REC_KEY)], shifts.at[span],
                        d_send.at[i], d_recv.at[k], {"sp": k},
                    ).wait_recv()
        total = squares[0, k, :1]
        for v in range(1, n):
            total = total + squares[v, k, :1]
        inv_rms = lax.rsqrt(total / gain_ref.shape[1] + EPS)
        inv_rms = jnp.transpose(jnp.broadcast_to(inv_rms, (128, rows)))
        for c in range(width // 128):
            lane = pl.ds(c * 128, 128)
            result = part[e, span, lane] + came[e, span, lane].astype(f32)
            x[span, lane] = (result * inv_rms).astype(bf16)
        heads[e, span, pl.ds(0, wide)] = stick_block(k, e, group, x, offset_ref)
        heads[e, span, pl.ds(wide, REC_VAL)] = state_block(
            k, e, x, att_width, bound_ref, shifts, rec_gain_ref, state
        )
        for i in range(2):
            @pl.when(s == ends[i])
            def _():
                for to in (range(n - 1, 0, -1) if i == 0 else range(n - 1)):
                    head_copy(i, k, to).start()

    def share_copy(k, b):
        to = lax.rem(t + b, nt)
        return remote(
            shares.at[k, to], landed.at[k, b], f_send.at[k, b], f_recv.at[k, b], {"tp": to}
        )

    def multiply(k):
        span = pl.ds(k * rows, rows)
        total = None
        for i in range(2):
            pl.when(s != ends[i])(lambda i=i: head_copy(i, k, ends[i]).wait_recv())
        for i in range(2):
            for ref, first, size in ((wa_ref, 0, wide), (wr_ref, wide, REC_VAL)):
                term = dot_nn(heads[i, span, pl.ds(first, size)], ref[pl.ds(i * size, size)])
                total = term if total is None else total + term
        shares[k] = total.astype(bf16).reshape(nt, piece, cols)
        for b in range(1, nt):
            share_copy(k, b).start()

    place = out_ref.at[:, pl.ds(pl.multiple_of(s * cols, cols), cols)]

    def final_copy(k):
        return remote(mixed.at[k], place, g_send.at[k], g_recv.at[s], {"sp": k})

    def final_here(k):
        return pltpu.make_async_copy(mixed.at[k], place, g_local)

    def combine(k):
        result = shares[k, t].astype(f32)
        for b in range(1, nt):
            share_copy(k, b).wait_recv()
            result = result + landed[k, b].astype(f32)
        mixed[k] = result.astype(bf16)
        pl.when(s != k)(lambda: final_copy(k).start())
        pl.when(s == k)(lambda: final_here(k).start())

    relay(0)
    for k in range(n):
        if k + 1 < n:
            relay(k + 1)
        project(k)

    @pl.when(jnp.logical_not(at_end))
    def _():
        for k in range(n):
            forward(k)

    @pl.when(at_end)
    def _():
        for k in range(n - 1):
            mix(k)

    multiply(0)

    @pl.when(at_end)
    def _():
        mix(n - 1)

    for k in range(1, n):
        multiply(k)
        combine(k - 1)
    combine(n - 1)

    for v in range(n):
        @pl.when(s != v)
        def _():
            remote(
                mixed.at[0], out_ref.at[:, pl.ds(v * cols, cols)], g_send.at[0], g_recv.at[v],
                {"sp": v},
            ).wait_recv()
        pl.when(s == v)(lambda v=v: final_here(v).wait())

    for j in range(nt):
        here = (s == t) & (t == j)
        pl.when(jnp.logical_not(here))(lambda j=j: first_copy(j).wait_send())
    for i in range(2):
        pl.when(s != ends[i])(lambda i=i: shift_copy(i).wait_send())
    for k in range(n):
        for d in range(1, nt):
            second_copy(k, d).wait_send()
            share_copy(k, d).wait_send()
        for i in range(2):
            pl.when(s != ends[i])(lambda i=i, k=k: square_copy(k, i).wait_send())

            @pl.when(s == ends[i])
            def _():
                for to in range(n):
                    if to != ends[i]:
                        head_copy(i, k, to).wait_send()

            @pl.when(s != ends[i])
            def _():
                for r in range(subs):
                    chain_copy(i, k * subs + r).wait_send()
        pl.when(s != k)(lambda k=k: final_copy(k).wait_send())


def stationary_fits(args):
    n, nt = lax.axis_size("sp"), lax.axis_size("tp")
    tokens, att_q, att_k, rec_i = args[0], args[2], args[3], args[7]
    rows, feats = tokens.shape
    return (
        n == nt
        and n >= 3
        and att_k.shape[0] // HEAD == 2
        and rec_i.shape[0] // REC_VAL == 2
        and (att_q.shape[0] // att_k.shape[0]) * HEAD == 128
        and feats == att_q.shape[1]
        and rows == 128
    )


def stationary(*args):
    n, nt = lax.axis_size("sp"), lax.axis_size("tp")
    tokens, norm_gain, att_q, att_k = args[:4]
    score_offset, lower_bound, decay_shift, rec_gain = args[10:]
    rows, feats = tokens.shape
    seq = rows * n
    cols = args[8].shape[1]
    group = att_q.shape[0] // att_k.shape[0]
    width = (group + 2) * HEAD + 2 * REC_KEY + REC_VAL
    wide = group * HEAD + REC_VAL
    piece = rows // nt
    chunks = seq // SUB
    bf16, f32 = jnp.bfloat16, jnp.float32
    dma = pltpu.SemaphoreType.DMA
    vmem = pl.BlockSpec(memory_space=pltpu.VMEM)
    smem = pl.BlockSpec(memory_space=pltpu.SMEM)
    return pl.pallas_call(
        functools.partial(layer_kernel, n, nt, group),
        out_shape=jax.ShapeDtypeStruct((piece, cols * n), bf16),
        in_specs=[vmem] * 11 + [smem, vmem, vmem],
        out_specs=vmem,
        scratch_shapes=[
            pltpu.VMEM((n, nt, piece, feats), bf16),
            pltpu.VMEM((seq, REC_KEY), f32),
            pltpu.VMEM((n, n, 8, rows), f32),
            pltpu.VMEM((2, seq, width), f32),
            pltpu.VMEM((2, seq, width), bf16),
            pltpu.VMEM((2, seq, width), bf16),
            pltpu.VMEM((seq, width), bf16),
            pltpu.VMEM((REC_VAL, REC_KEY), f32),
            pltpu.VMEM((2, seq, wide), bf16),
            pltpu.VMEM((n, nt, piece, cols), bf16),
            pltpu.VMEM((n, nt, piece, cols), bf16),
            pltpu.VMEM((n, piece, cols), bf16),
            dma((nt,)), dma((n,)), dma, dma((n, nt)), dma((n, nt)), dma((2,)), dma((n,)), dma,
            dma((n, 2)), dma((n, n)), dma((2, chunks)), dma((2, chunks)),
            dma((n, n)), dma((2, n)), dma((n, nt)), dma((n, nt)), dma((n,)), dma((n,)), dma,
        ],
        compiler_params=pltpu.CompilerParams(collective_id=0, has_side_effects=True),
        name="layer",
    )(
        tokens, norm_gain.reshape(1, -1), *args[2:8], decay_shift, args[8], args[9],
        score_offset, lower_bound.reshape(1, -1), rec_gain.reshape(1, -1),
    )


def on_device(*args):
    if stationary_fits(args):
        return stationary(*args)
    return gathered_plan(*args)


def solution(mesh):
    in_specs = (
        P(("grp", "sp"), "tp"),
        P(),
        P("tp", "sp"),
        P("tp", "sp"),
        P("tp", "sp"),
        P("tp", "sp"),
        P("tp", "sp"),
        P("tp", "sp"),
        P("tp", "sp"),
        P("tp", "sp"),
        P("tp"),
        P("tp"),
        P(("grp", "sp"), "tp"),
        P("tp"),
    )
    out_specs = P(("grp", "sp", "tp"), None)
    return jax.shard_map(
        on_device, mesh=mesh, in_specs=in_specs, out_specs=out_specs, check_vma=False
    )
```

```python
import functools

import jax
import jax.numpy as jnp
from jax import lax
from jax.experimental import pallas as pl
from jax.experimental.pallas import tpu as pltpu
from jax.sharding import PartitionSpec as P

HEAD = 64
REC_KEY = 128
REC_VAL = 128
SPAN = 64


EPS = 1e-06
TOP_PRECISION = lax.Precision.HIGHEST


def entering(x, axis, combine, identity):
    count, here = (lax.axis_size(axis), lax.axis_index(axis))
    everything = jax.tree.map(
        lambda part, kind: lax.all_gather(part.astype(kind), axis), x, (jnp.bfloat16, jnp.bfloat16)
    )
    start = jax.tree.map(
        lambda part, zero: jnp.broadcast_to(jnp.asarray(zero, part.dtype), part.shape), x, identity
    )

    def entering_turn(k, before):
        reached = k < here
        new = combine(
            before, jax.tree.map(lambda part, own: part[k].astype(own.dtype), everything, x)
        )
        return jax.tree.map(lambda a, b: jnp.where(reached, a, b), new, before)

    return lax.fori_loop(0, count, entering_turn, start)


def make_fold(norm_gain, weights, carry, piece):
    elementwise_sq, totals = carry
    raw = piece.astype(jnp.float32)
    scaled = (raw * norm_gain[None, :]).astype(jnp.bfloat16)
    elementwise_sq = jnp.sum(raw * raw, axis=1)
    updated = []
    for total, weight in zip(totals, weights):
        updated.append(
            lax.dot_general(
                scaled, weight, (((1,), (1,)), ((), ())), preferred_element_type=jnp.float32
            )
        )
    return (elementwise_sq, tuple(updated))


def project_all(tokens, norm_gain, weights):
    rows = tokens.shape[0]
    width = weights[0].shape[1]
    start_carry = (
        jnp.zeros((rows,), jnp.float32),
        tuple((jnp.zeros((rows, weight.shape[0]), jnp.float32) for weight in weights)),
    )
    elementwise_sq, totals = make_fold(
        norm_gain, weights, start_carry, lax.all_gather(tokens, "tp", axis=1, tiled=True)
    )
    inv_rms = lax.rsqrt(elementwise_sq / width + EPS)
    return tuple((total * inv_rms[:, None] for total in totals))


def attention(att_query, key_value, score_offset):
    rows = att_query.shape[0]
    gathered = lax.all_gather(key_value, "sp", axis=0, tiled=True)
    seq = gathered.shape[0]
    kv_heads = key_value.shape[1] // (2 * HEAD)
    q_heads = att_query.shape[1] // HEAD
    group = q_heads // kv_heads
    kv_width = kv_heads * HEAD
    queries = att_query.reshape(rows, kv_heads, group, HEAD)
    offsets = score_offset.reshape(kv_heads, group)
    kblock = min(1024, seq)
    first_row = lax.axis_index("sp") * rows
    query_pos = first_row + jnp.arange(rows, dtype=jnp.int32)
    count = (first_row + rows - 1) // kblock + 1

    def attention_turn(step, carry):
        summed, run = carry
        block_start = (count - 1 - step) * kblock
        block = lax.dynamic_slice_in_dim(gathered, block_start, kblock, 0)
        keys = block[:, :kv_width].reshape(kblock, kv_heads, HEAD)
        values = block[:, kv_width:].reshape(kblock, kv_heads, HEAD)
        score = (
            jnp.einsum("tkgd,skd->tkgs", queries, keys, preferred_element_type=jnp.float32)
            * HEAD ** (-0.5)
            + offsets[None, :, :, None]
        )
        key_pos = block_start + jnp.arange(kblock, dtype=jnp.int32)
        visible = (key_pos[None, :] < query_pos[:, None])[:, None, None, :]
        keep = jnp.where(visible, jax.nn.log_sigmoid(-score), 0.0)
        tail = lax.cumsum(keep, axis=3, reverse=True) - keep
        weight = jnp.where(
            visible, jnp.exp(jax.nn.log_sigmoid(score) + tail + run[..., None]), 0.0
        ).astype(jnp.bfloat16)
        summed = summed + jnp.einsum(
            "tkgs,skd->tkgd", weight, values, preferred_element_type=jnp.float32
        )
        return (summed, run + jnp.sum(keep, axis=3))

    start_carry = (
        jnp.zeros((rows, kv_heads, group, HEAD), jnp.float32),
        jnp.zeros((rows, kv_heads, group), jnp.float32),
    )
    summed, _ = lax.fori_loop(0, count, attention_turn, start_carry)
    return summed.reshape(rows, q_heads * HEAD).astype(jnp.bfloat16)


def block_pass(carry, inputs):
    state_matrix, prefix = carry
    query_rows, log_decay, keyed_values, value_rows = inputs
    span = query_rows.shape[0]
    cumulative_log = jnp.cumsum(log_decay, axis=0)
    lower = jnp.arange(span, dtype=jnp.int32)[:, None] >= jnp.arange(span, dtype=jnp.int32)[None, :]
    diff = cumulative_log[:, None] - cumulative_log[None, :]
    decay = jnp.exp(jnp.where(lower[:, :, None, None], diff, -jnp.inf))
    score = jnp.einsum(
        "thk,tshk,shk->ths", query_rows, decay, keyed_values, precision=TOP_PRECISION
    )
    inner = jnp.einsum("ths,shv->thv", score, value_rows, precision=TOP_PRECISION)
    outer_product = jnp.einsum(
        "ril,ilc->ric", query_rows * jnp.exp(cumulative_log), state_matrix, precision=TOP_PRECISION
    )
    final_state = cumulative_log[-1]
    state_matrix = state_matrix * jnp.exp(final_state)[:, :, None] + jnp.einsum(
        "iag,iax->agx",
        keyed_values * jnp.exp(final_state[None] - cumulative_log),
        value_rows,
        precision=TOP_PRECISION,
    )
    reach_limit = query_rows * jnp.exp(cumulative_log + prefix[None])
    return ((state_matrix, prefix + final_state), (inner + outer_product, reach_limit))


def chain(earlier, later):
    return (earlier[0] * later[0], earlier[1] * later[0][:, :, None] + later[1])


def recurrence(rec_query, rec_forget, rec_input, lower_bound, decay_shift, rec_gain):
    rows = rec_query.shape[0]
    heads = rec_gain.shape[0] // REC_VAL
    logit = rec_forget.astype(jnp.float32)
    gap = 1.0 - lower_bound
    log_decay = jnp.log(lower_bound + gap * jax.nn.sigmoid(logit)) + decay_shift
    keyed_values = gap * jax.nn.sigmoid(-logit)
    query_rows = jax.nn.silu(rec_query.astype(jnp.float32))
    blocks = rows // SPAN

    def split(array, depth):
        return array.reshape(blocks, SPAN, heads, depth)

    start_carry = (
        jnp.zeros((heads, REC_KEY, REC_VAL), jnp.float32),
        jnp.zeros((heads, REC_KEY), jnp.float32),
    )
    (state_matrix, total), (local, reach_limit) = lax.scan(
        block_pass,
        start_carry,
        (
            split(query_rows, REC_KEY),
            split(log_decay, REC_KEY),
            split(keyed_values, REC_KEY),
            split(rec_input.astype(jnp.float32), REC_VAL),
        ),
    )
    identity = (
        jnp.ones((heads, REC_KEY), jnp.float32),
        jnp.zeros((heads, REC_KEY, REC_VAL), jnp.float32),
    )
    incoming_state = entering((jnp.exp(total), state_matrix), "sp", chain, identity)
    running_memory = jnp.einsum(
        "lida,dao->lido", reach_limit, incoming_state[1], precision=TOP_PRECISION
    )
    rec_raw = (local + running_memory).reshape(rows, heads, REC_VAL)
    rescaled_input = (
        rec_raw
        * lax.rsqrt(jnp.mean(rec_raw * rec_raw, axis=2, keepdims=True) + EPS)
        * rec_gain.reshape(heads, REC_VAL)
    )
    return rescaled_input.reshape(rows, heads * REC_VAL).astype(jnp.bfloat16)


def gathered_plan(
    tokens,
    norm_gain,
    att_q_weight,
    att_k_weight,
    att_v_weight,
    rec_q_weight,
    rec_f_weight,
    rec_i_weight,
    att_out_weight,
    rec_out_weight,
    score_offset,
    lower_bound,
    decay_shift,
    rec_gain,
):
    inputs = (
        lax.all_gather(att_q_weight, "sp", axis=1, tiled=True),
        lax.all_gather(att_k_weight, "sp", axis=1, tiled=True),
        lax.all_gather(att_v_weight, "sp", axis=1, tiled=True),
        lax.all_gather(rec_q_weight, "sp", axis=1, tiled=True),
        lax.all_gather(rec_f_weight, "sp", axis=1, tiled=True),
        lax.all_gather(rec_i_weight, "sp", axis=1, tiled=True),
    )
    projected = project_all(tokens, norm_gain, inputs)
    att_query = projected[0].astype(jnp.bfloat16)
    key_value = jnp.concatenate(projected[1:3], axis=1).astype(jnp.bfloat16)
    rec_query = projected[3].astype(jnp.bfloat16)
    rec_forget = projected[4].astype(jnp.bfloat16)
    rec_input = projected[5].astype(jnp.bfloat16)
    att_out = attention(att_query, key_value, score_offset)
    rec_out = recurrence(rec_query, rec_forget, rec_input, lower_bound, decay_shift, rec_gain)
    outputs = (
        lax.all_gather(att_out_weight, "sp", axis=1, tiled=True),
        lax.all_gather(rec_out_weight, "sp", axis=1, tiled=True),
    )
    att_rows, rec_rows = outputs
    return lax.psum_scatter(
        (
            jnp.dot(att_out, att_rows, preferred_element_type=jnp.float32)
            + jnp.dot(rec_out, rec_rows, preferred_element_type=jnp.float32)
        ).astype(jnp.bfloat16),
        "tp",
        scatter_dimension=0,
        tiled=True,
    )


MESH = pl.DeviceIdType.MESH
STEP = 32


def dot_nt(a, b):
    return lax.dot_general(a, b, (((1,), (1,)), ((), ())), preferred_element_type=jnp.float32)


def dot_tn(a, b):
    return lax.dot_general(a, b, (((0,), (0,)), ((), ())), preferred_element_type=jnp.float32)


def dot_nn(a, b):
    return jnp.dot(a, b, preferred_element_type=jnp.float32)


def remote(src, dst, send_sem, recv_sem, target):
    return pltpu.make_async_remote_copy(
        src_ref=src,
        dst_ref=dst,
        send_sem=send_sem,
        recv_sem=recv_sem,
        device_id=target,
        device_id_type=MESH,
    )


SUB = 32
LAG = 3.5


def stick_block(q, j, group, x, offset_ref):
    block = 128
    low = lax.broadcasted_iota(jnp.int32, (block, block), 0)
    high = lax.broadcasted_iota(jnp.int32, (block, block), 1)
    later = (low > high).astype(jnp.bfloat16)
    visible = jnp.concatenate([high < low] * group, axis=0)
    offset = jnp.concatenate(
        [jnp.full((block, block), offset_ref[j * group + g], jnp.float32) for g in range(group)],
        axis=0,
    )
    queries = x[q * block:(q + 1) * block, :group * HEAD]
    queries = jnp.concatenate([queries[:, g * HEAD:(g + 1) * HEAD] for g in range(group)], axis=0)
    run = jnp.zeros((group * block, 1), jnp.float32)
    summed = jnp.zeros((group * block, HEAD), jnp.float32)
    for c in range(q, -1, -1):
        keys = x[c * block:(c + 1) * block, group * HEAD:(group + 1) * HEAD]
        values = x[c * block:(c + 1) * block, (group + 1) * HEAD:(group + 2) * HEAD]
        score = dot_nt(queries, keys) * HEAD ** (-0.5) + offset
        keep = -(jnp.maximum(score, 0.0) + jnp.log1p(jnp.exp(-jnp.abs(score))))
        gate = score + keep
        if c == q:
            keep = jnp.where(visible, keep, 0.0)
        top = keep.astype(jnp.bfloat16)
        rest = (keep - top.astype(jnp.float32)).astype(jnp.bfloat16)
        tail = dot_nn(top, later) + dot_nn(rest, later)
        weight = jnp.exp(gate + tail + run)
        if c == q:
            weight = jnp.where(visible, weight, 0.0)
        summed = summed + dot_nn(weight.astype(jnp.bfloat16), values)
        run = run + jnp.sum(keep, axis=1, keepdims=True)
    return jnp.concatenate(
        [summed[g * block:(g + 1) * block] for g in range(group)], axis=1
    ).astype(jnp.bfloat16)


def state_block(b, j, x, first, bound_ref, shift_ref, gain_ref, state_ref):
    block = 128
    bound = bound_ref[:, pl.ds(pl.multiple_of(j * REC_KEY, REC_KEY), REC_KEY)]
    gain = gain_ref[:, pl.ds(pl.multiple_of(j * REC_VAL, REC_VAL), REC_VAL)]
    gap = 1.0 - bound
    low = lax.broadcasted_iota(jnp.int32, (block, block), 0)
    high = lax.broadcasted_iota(jnp.int32, (block, block), 1)
    upto = ((high <= low) & (high // STEP == low // STEP)).astype(jnp.float32)
    lower = (
        lax.broadcasted_iota(jnp.int32, (STEP, STEP), 0)
        >= lax.broadcasted_iota(jnp.int32, (STEP, STEP), 1)
    )
    state = jnp.zeros((REC_VAL, REC_KEY), jnp.float32) if b == 0 else state_ref[...]
    at = slice(b * block, (b + 1) * block)
    query = x[at, first:first + REC_KEY].astype(jnp.float32)
    logit = x[at, first + REC_KEY:first + 2 * REC_KEY].astype(jnp.float32)
    value = x[at, first + 2 * REC_KEY:first + 2 * REC_KEY + REC_VAL]
    log_decay = jnp.log(bound + gap * jax.nn.sigmoid(logit)) + shift_ref[at]
    keyed = gap * jax.nn.sigmoid(-logit)
    query = query * jax.nn.sigmoid(query)
    running = jnp.dot(upto, log_decay, precision=TOP_PRECISION, preferred_element_type=jnp.float32)
    outs = []
    for i in range(block // STEP):
        it = slice(i * STEP, (i + 1) * STEP)
        cumulative, q, k, v = running[it], query[it], keyed[it], value[it]
        middle = cumulative[STEP // 2 - 1:STEP // 2]
        last = cumulative[STEP - 1:STEP]
        score = dot_nt(
            (q * jnp.exp(cumulative - middle)).astype(jnp.bfloat16),
            (k * jnp.exp(middle - cumulative)).astype(jnp.bfloat16),
        )
        score = jnp.where(lower, score, 0.0).astype(jnp.bfloat16)
        raw = dot_nn(score, v) + dot_nt(
            (q * jnp.exp(cumulative)).astype(jnp.bfloat16), state.astype(jnp.bfloat16)
        )
        state = state * jnp.exp(last) + dot_tn(
            v, (k * jnp.exp(last - cumulative)).astype(jnp.bfloat16)
        )
        scale = lax.rsqrt(jnp.mean(raw * raw, axis=1, keepdims=True) + EPS)
        outs.append((raw * scale * gain).astype(jnp.bfloat16))
    state_ref[...] = state
    return jnp.concatenate(outs, axis=0)


def layer_kernel(
    n, nt, group,
    tok_ref, gain_ref, aq_ref, ak_ref, av_ref, rq_ref, rf_ref, ri_ref, shift_ref,
    wa_ref, wr_ref, offset_ref, bound_ref, rec_gain_ref,
    out_ref,
    tbuf, shifts, squares, part, sent, came, x, state, heads, shares, landed, mixed,
    a_send, a_recv, a_local, b_send, b_recv, d_send, d_recv, d_local, q_send, q_recv,
    c_send, c_recv, e_send, e_recv, f_send, f_recv, g_send, g_recv, g_local,
):
    s, t = lax.axis_index("sp"), lax.axis_index("tp")
    rows, feats = tok_ref.shape
    piece = rows // nt
    width = x.shape[1]
    att_width = (group + 2) * HEAD
    wide = group * HEAD
    cols = wa_ref.shape[1]
    subs = rows // SUB
    ends = (0, n - 1)
    at_end = (s == 0) | (s == n - 1)
    e = s // (n - 1)
    f32, bf16 = jnp.float32, jnp.bfloat16

    barrier = pltpu.get_barrier_semaphore()
    for a in range(n):
        for b in range(nt):
            if a or b:
                pl.semaphore_signal(
                    barrier, inc=1,
                    device_id={"sp": lax.rem(s + a, n), "tp": lax.rem(t + b, nt)},
                    device_id_type=MESH,
                )
    pl.semaphore_wait(barrier, n * nt - 1)

    def first_copy(j):
        return remote(
            tok_ref.at[pl.ds(j * piece, piece)], tbuf.at[s, j], a_send.at[j], a_recv.at[s],
            {"sp": t, "tp": j},
        )

    def first_here(j):
        return pltpu.make_async_copy(
            tok_ref.at[pl.ds(j * piece, piece)], tbuf.at[s, j], a_local
        )

    for j in range(nt):
        here = (s == t) & (t == j)
        pl.when(jnp.logical_not(here))(lambda j=j: first_copy(j).start())
        pl.when(here)(lambda j=j: first_here(j).start())

    def shift_copy(i):
        return remote(
            shift_ref.at[:, pl.ds(i * REC_KEY, REC_KEY)], shifts.at[pl.ds(s * rows, rows)],
            d_send.at[i], d_recv.at[s], {"sp": ends[i]},
        )

    def shift_here(i):
        return pltpu.make_async_copy(
            shift_ref.at[:, pl.ds(i * REC_KEY, REC_KEY)], shifts.at[pl.ds(s * rows, rows)], d_local
        )

    def second_copy(k, d):
        return remote(
            tbuf.at[k, t], tbuf.at[k, t], b_send.at[k, d], b_recv.at[k, d],
            {"tp": lax.rem(t + d, nt)},
        )

    def relay(k):
        here = (s == k) & (t == k)

        def arrived():
            remote(
                tok_ref.at[pl.ds(0, piece)], tbuf.at[k, t], a_send.at[0], a_recv.at[k],
                {"sp": t, "tp": t},
            ).wait_recv()

        pl.when(jnp.logical_not(here))(arrived)
        pl.when(here)(lambda: first_here(k).wait())
        for d in range(1, nt):
            second_copy(k, d).start()

    gain = gain_ref[:, pl.ds(pl.multiple_of(s * feats, feats), feats)]

    def square_copy(k, i):
        return remote(
            squares.at[s, k], squares.at[s, k], q_send.at[k, i], q_recv.at[s, k], {"sp": ends[i]}
        )

    def chain_copy(i, c):
        to = jnp.maximum(s - 1, 0) if i == 0 else jnp.minimum(s + 1, n - 1)
        return remote(
            sent.at[i, pl.ds(c * SUB, SUB)], came.at[i, pl.ds(c * SUB, SUB)],
            c_send.at[i, c], c_recv.at[i, c], {"sp": to},
        )

    weights = []
    for i in range(2):
        weights.append(jnp.concatenate(
            [
                aq_ref[pl.ds(i * wide, wide)],
                ak_ref[pl.ds(i * HEAD, HEAD)],
                av_ref[pl.ds(i * HEAD, HEAD)],
                rq_ref[pl.ds(i * REC_KEY, REC_KEY)],
                rf_ref[pl.ds(i * REC_KEY, REC_KEY)],
                ri_ref[pl.ds(i * REC_VAL, REC_VAL)],
            ],
            axis=0,
        ))

    def project(k):
        for d in range(1, nt):
            second_copy(k, d).wait_recv()
        raw = tbuf[k].reshape(rows, feats).astype(f32)
        scaled = (raw * gain).astype(bf16)
        for i in range(2):
            product = dot_nt(scaled, weights[i])
            part[i, pl.ds(k * rows, rows)] = product

            @pl.when(s == ends[1 - i])
            def _():
                for r in range(subs):
                    c = k * subs + r
                    sent[i, pl.ds(c * SUB, SUB)] = product[r * SUB:(r + 1) * SUB].astype(bf16)
                    chain_copy(i, c).start()

        total = jnp.sum(raw * raw, axis=1, keepdims=True)
        flat = jnp.transpose(jnp.broadcast_to(total, (rows, 128)))
        squares[s, k] = flat[:8]
        for i in range(2):
            pl.when(s != ends[i])(lambda i=i: square_copy(k, i).start())

    def forward(i, c):
        chain_copy(i, c).wait_recv()
        at = (i, pl.ds(c * SUB, SUB))
        sent[at] = (part[at] + came[at].astype(f32)).astype(bf16)
        chain_copy(i, c).start()

    def head_copy(i, k, to):
        at = (i, pl.ds(k * rows, rows))
        return remote(
            heads.at[at], heads.at[at], e_send.at[k, to], e_recv.at[i, k], {"sp": to}
        )

    def mix(k):
        span = pl.ds(k * rows, rows)
        for i in range(2):
            @pl.when(s == ends[i])
            def _():
                for r in range(subs):
                    chain_copy(i, k * subs + r).wait_recv()
                for v in range(n):
                    if v != ends[i]:
                        remote(
                            squares.at[v, k], squares.at[v, k], q_send.at[k, i], q_recv.at[v, k],
                            {"sp": v},
                        ).wait_recv()
                if k == ends[i]:
                    shift_here(i).wait()
                else:
                    remote(
                        shift_ref.at[:, pl.ds(i * REC_KEY, REC_KEY)], shifts.at[span],
                        d_send.at[i], d_recv.at[k], {"sp": k},
                    ).wait_recv()
        total = squares[0, k, :1]
        for v in range(1, n):
            total = total + squares[v, k, :1]
        inv_rms = lax.rsqrt(total / gain_ref.shape[1] + EPS)
        inv_rms = jnp.transpose(jnp.broadcast_to(inv_rms, (128, rows)))
        for c in range(width // 128):
            lane = pl.ds(c * 128, 128)
            result = part[e, span, lane] + came[e, span, lane].astype(f32)
            x[span, lane] = (result * inv_rms).astype(bf16)
        heads[e, span, pl.ds(0, wide)] = stick_block(k, e, group, x, offset_ref)
        heads[e, span, pl.ds(wide, REC_VAL)] = state_block(
            k, e, x, att_width, bound_ref, shifts, rec_gain_ref, state
        )
        for i in range(2):
            @pl.when(s == ends[i])
            def _():
                for to in (range(n - 1, 0, -1) if i == 0 else range(n - 1)):
                    head_copy(i, k, to).start()

    def share_copy(k, b):
        to = lax.rem(t + b, nt)
        return remote(
            shares.at[k, to], landed.at[k, b], f_send.at[k, b], f_recv.at[k, b], {"tp": to}
        )

    def multiply(k):
        span = pl.ds(k * rows, rows)
        total = None
        for i in range(2):
            pl.when(s != ends[i])(lambda i=i: head_copy(i, k, ends[i]).wait_recv())
        for i in range(2):
            for ref, first, size in ((wa_ref, 0, wide), (wr_ref, wide, REC_VAL)):
                term = dot_nn(heads[i, span, pl.ds(first, size)], ref[pl.ds(i * size, size)])
                total = term if total is None else total + term
        shares[k] = total.astype(bf16).reshape(nt, piece, cols)
        for b in range(1, nt):
            share_copy(k, b).start()

    place = out_ref.at[:, pl.ds(pl.multiple_of(s * cols, cols), cols)]

    def final_copy(k):
        return remote(mixed.at[k], place, g_send.at[k], g_recv.at[s], {"sp": k})

    def final_here(k):
        return pltpu.make_async_copy(mixed.at[k], place, g_local)

    def combine(k):
        result = shares[k, t].astype(f32)
        for b in range(1, nt):
            share_copy(k, b).wait_recv()
            result = result + landed[k, b].astype(f32)
        mixed[k] = result.astype(bf16)
        pl.when(s != k)(lambda: final_copy(k).start())
        pl.when(s == k)(lambda: final_here(k).start())

    relay(0)
    for k in range(n):
        if k + 1 < n:
            relay(k + 1)
        project(k)
        if k == 0:
            for i, u in enumerate(ends):
                pl.when(s != u)(lambda i=i: shift_copy(i).start())
                pl.when(s == u)(lambda i=i: shift_here(i).start())

    for v in range(1, n - 1):
        events = [(c + LAG * v, 1, c) for c in range(n * subs)]
        events += [(c + LAG * (n - 1 - v), 0, c) for c in range(n * subs)]

        @pl.when(s == v)
        def _():
            for _, i, c in sorted(events):
                forward(i, c)

    @pl.when(at_end)
    def _():
        for k in range(n - 1):
            mix(k)

    multiply(0)

    @pl.when(at_end)
    def _():
        mix(n - 1)

    for k in range(1, n):
        multiply(k)
        combine(k - 1)
    combine(n - 1)

    for v in range(n):
        @pl.when(s != v)
        def _():
            remote(
                mixed.at[0], out_ref.at[:, pl.ds(v * cols, cols)], g_send.at[0], g_recv.at[v],
                {"sp": v},
            ).wait_recv()
        pl.when(s == v)(lambda v=v: final_here(v).wait())

    for j in range(nt):
        here = (s == t) & (t == j)
        pl.when(jnp.logical_not(here))(lambda j=j: first_copy(j).wait_send())
    for i in range(2):
        pl.when(s != ends[i])(lambda i=i: shift_copy(i).wait_send())
    for k in range(n):
        for d in range(1, nt):
            second_copy(k, d).wait_send()
            share_copy(k, d).wait_send()
        for i in range(2):
            pl.when(s != ends[i])(lambda i=i, k=k: square_copy(k, i).wait_send())

            @pl.when(s == ends[i])
            def _():
                for to in range(n):
                    if to != ends[i]:
                        head_copy(i, k, to).wait_send()

            @pl.when(s != ends[i])
            def _():
                for r in range(subs):
                    chain_copy(i, k * subs + r).wait_send()
        pl.when(s != k)(lambda k=k: final_copy(k).wait_send())


def stationary_fits(args):
    n, nt = lax.axis_size("sp"), lax.axis_size("tp")
    tokens, att_q, att_k, rec_i = args[0], args[2], args[3], args[7]
    rows, feats = tokens.shape
    return (
        n == nt
        and n >= 3
        and att_k.shape[0] // HEAD == 2
        and rec_i.shape[0] // REC_VAL == 2
        and (att_q.shape[0] // att_k.shape[0]) * HEAD == 128
        and feats == att_q.shape[1]
        and rows == 128
    )


def stationary(*args):
    n, nt = lax.axis_size("sp"), lax.axis_size("tp")
    tokens, norm_gain, att_q, att_k = args[:4]
    score_offset, lower_bound, decay_shift, rec_gain = args[10:]
    rows, feats = tokens.shape
    seq = rows * n
    cols = args[8].shape[1]
    group = att_q.shape[0] // att_k.shape[0]
    width = (group + 2) * HEAD + 2 * REC_KEY + REC_VAL
    wide = group * HEAD + REC_VAL
    piece = rows // nt
    chunks = seq // SUB
    bf16, f32 = jnp.bfloat16, jnp.float32
    dma = pltpu.SemaphoreType.DMA
    vmem = pl.BlockSpec(memory_space=pltpu.VMEM)
    smem = pl.BlockSpec(memory_space=pltpu.SMEM)
    return pl.pallas_call(
        functools.partial(layer_kernel, n, nt, group),
        out_shape=jax.ShapeDtypeStruct((piece, cols * n), bf16),
        in_specs=[vmem] * 11 + [smem, vmem, vmem],
        out_specs=vmem,
        scratch_shapes=[
            pltpu.VMEM((n, nt, piece, feats), bf16),
            pltpu.VMEM((seq, REC_KEY), f32),
            pltpu.VMEM((n, n, 8, rows), f32),
            pltpu.VMEM((2, seq, width), f32),
            pltpu.VMEM((2, seq, width), bf16),
            pltpu.VMEM((2, seq, width), bf16),
            pltpu.VMEM((seq, width), bf16),
            pltpu.VMEM((REC_VAL, REC_KEY), f32),
            pltpu.VMEM((2, seq, wide), bf16),
            pltpu.VMEM((n, nt, piece, cols), bf16),
            pltpu.VMEM((n, nt, piece, cols), bf16),
            pltpu.VMEM((n, piece, cols), bf16),
            dma((nt,)), dma((n,)), dma, dma((n, nt)), dma((n, nt)), dma((2,)), dma((n,)), dma,
            dma((n, 2)), dma((n, n)), dma((2, chunks)), dma((2, chunks)),
            dma((n, n)), dma((2, n)), dma((n, nt)), dma((n, nt)), dma((n,)), dma((n,)), dma,
        ],
        compiler_params=pltpu.CompilerParams(collective_id=0, has_side_effects=True),
        name="layer",
    )(
        tokens, norm_gain.reshape(1, -1), *args[2:8], decay_shift, args[8], args[9],
        score_offset, lower_bound.reshape(1, -1), rec_gain.reshape(1, -1),
    )


def on_device(*args):
    if stationary_fits(args):
        return stationary(*args)
    return gathered_plan(*args)


def solution(mesh):
    in_specs = (
        P(("grp", "sp"), "tp"),
        P(),
        P("tp", "sp"),
        P("tp", "sp"),
        P("tp", "sp"),
        P("tp", "sp"),
        P("tp", "sp"),
        P("tp", "sp"),
        P("tp", "sp"),
        P("tp", "sp"),
        P("tp"),
        P("tp"),
        P(("grp", "sp"), "tp"),
        P("tp"),
    )
    out_specs = P(("grp", "sp", "tp"), None)
    return jax.shard_map(
        on_device, mesh=mesh, in_specs=in_specs, out_specs=out_specs, check_vma=False
    )
```
